32 devices in a mesh: sp: 8 (over z, x), tp: 4 (over y, core).
Axes of the slice: x: 2, y: 2, z: 4, core: 2. Of those that a mesh axis runs over, the one named last changes fastest.
Arguments:
- target: bfloat16 [1024, 4096], P('sp', 'tp'), may hold values from -300 to 300
- gain: float32 [4096], P('tp'), may hold values from 0.1 to 1.9
- w_query: bfloat16 [4096, 4096], P('tp'), may hold values from -0.09375 to 0.09375
- queries: bfloat16 [1024, 4096], P('sp', 'tp'), may hold values from -13 to 13
- keys: bfloat16 [4096, 1024], P('sp'), may hold values from -4 to 4
- values: bfloat16 [4096, 1024], P('sp'), may hold values from -4 to 4
- attn_out: bfloat16 [1024, 4096], P('sp', 'tp'), may hold values from -4 to 4
- grad_out: bfloat16 [1024, 4096], P('sp', 'tp'), may hold values from -64 to 64
Outputs:
- grad_rows: bfloat16 [1024, 4096], P('sp', 'tp')
- grad_weight: float32 [4096, 4096], P(('tp', 'sp'))
- grad_keys: float32 [4096, 1024], P(('sp', 'tp'))
- grad_values: float32 [4096, 1024], P(('sp', 'tp'))
The draws below stay inside these ranges and needn't reach their ends.
All inputs are finite; a program needn't handle non-finite values.
Results may differ from the reference program's by a relative error of at most 0.018.
Values may be sent and summed in bfloat16 or wider, within the bound.
A program may use at most 64 MiB of HBM per device.

```python
import math
import jax
import jax.numpy as jnp
from jax import lax

WIDTH = 4096
HEADS = 16
KV_HEADS = 4
HEAD_DIM = 256
TARGET_ROWS = 1024
SOURCE_ROWS = 4096


def draw_target(key, part):
    base_key = jax.random.fold_in(key, 11)
    row_key = jax.random.fold_in(key, 12)
    col_key = jax.random.fold_in(key, 13)
    array_shape = (TARGET_ROWS, WIDTH)
    base_draw = jnp.clip(jax.random.normal(base_key, array_shape, jnp.float32), -4.0, 4.0)
    row_scale = jnp.exp(jax.random.uniform(row_key, (TARGET_ROWS, 1), jnp.float32, 0.0, math.log(10.0)))
    column_ramp = jnp.exp(math.log(5.0) * jnp.arange(WIDTH, dtype=jnp.float32) / WIDTH)
    col_scale = column_ramp * jax.random.uniform(col_key, (WIDTH,), jnp.float32, 0.5, 1.5)
    return (base_draw * row_scale * col_scale).astype(jnp.bfloat16)


def draw_keys(key, part):
    base_key = jax.random.fold_in(key, 21)
    array_shape = (SOURCE_ROWS, KV_HEADS * HEAD_DIM)
    drawn = jnp.clip(jax.random.normal(base_key, array_shape, jnp.float32), -4.0, 4.0)
    return drawn.astype(jnp.bfloat16)


def draw_queries(key, part):
    base_key = jax.random.fold_in(key, 31)
    array_shape = (TARGET_ROWS, HEADS * HEAD_DIM)
    drawn = jnp.clip(jax.random.normal(base_key, array_shape, jnp.float32), -4.0, 4.0)
    return drawn.astype(jnp.bfloat16)


def steps_of(stream_key, shape, cuts, low, top_value):
    level, own = 1.0, jax.random.fold_in(stream_key, 6)
    for axis_at, shards_of in cuts:
        heights = jnp.exp(jax.random.uniform(jax.random.fold_in(own, axis_at), (shards_of,), jnp.float32, low / len(cuts), top_value / len(cuts)))
        level = level * jnp.repeat(heights, shape[axis_at] // shards_of).reshape([-1 if axis == axis_at else 1 for axis in range(len(shape))])
    return level


def scatter_about(own_key, dims, scale, limit, shards=(), held_as=jnp.bfloat16):
    level = steps_of(own_key, dims, shards, -0.22, 0.18) if shards else 1.0
    values = jax.random.normal(own_key, dims, jnp.float32) * scale * level
    return jnp.minimum(jnp.maximum(values, -limit), limit).astype(held_as)


def setup_inputs(seed: int = 0) -> dict:
    seeds = jax.random.split(jax.random.key(seed), 9)
    return {
        "target": draw_target(jax.random.fold_in(seeds[8], 71), 0),
        "gain": jnp.clip(1.0 + 0.18 * jax.random.normal(seeds[1], (WIDTH,), jnp.float32), 0.1, 1.9),
        "w_query": scatter_about(seeds[2], (WIDTH, HEADS * HEAD_DIM), WIDTH ** -0.5, 0.09375, ((0, 4),)),
        "queries": draw_queries(jax.random.fold_in(seeds[8], 71), 0),
        "keys": draw_keys(jax.random.fold_in(seeds[8], 71), 0),
        "values": scatter_about(seeds[5], (SOURCE_ROWS, KV_HEADS * HEAD_DIM), 1.0, 4.0, ((0, 8),)),
        "attn_out": scatter_about(seeds[6], (TARGET_ROWS, HEADS * HEAD_DIM), 1.0, 4.0, ((0, 8), (1, 4))),
        "grad_out": scatter_about(seeds[7], (TARGET_ROWS, HEADS * HEAD_DIM), 16.0, 64.0, ((0, 8), (1, 4))),
    }


norm_eps = 1e-06

def reference(target, gain, w_query, queries, keys, values, attn_out, grad_out):
    target_wide = target.astype(jnp.float32)
    inverse = lax.rsqrt(lax.optimization_barrier(jnp.mean(target_wide * target_wide, axis=1)) + norm_eps)
    normed = (target_wide * inverse[:, None] * gain).astype(jnp.bfloat16)
    group_size = HEADS // KV_HEADS
    score_scale = HEAD_DIM ** (-0.5)
    row_count = queries.shape[0]
    source_count = keys.shape[0]
    query_heads = queries.reshape(row_count, HEADS, HEAD_DIM).transpose(1, 0, 2)
    grad_heads = grad_out.reshape(row_count, HEADS, HEAD_DIM).transpose(1, 0, 2)
    out_heads = attn_out.reshape(row_count, HEADS, HEAD_DIM).transpose(1, 0, 2)
    deltas = lax.optimization_barrier(jnp.sum(grad_heads.astype(jnp.float32) * out_heads.astype(jnp.float32), axis=2))
    head_ids = jnp.arange(HEADS, dtype=jnp.int32)

    def one_head(inputs):
        query_head, grad_head, delta_head, head_id = inputs
        kv_start = (head_id // group_size * HEAD_DIM).astype(jnp.int32)
        key_head = lax.dynamic_slice_in_dim(keys, kv_start, HEAD_DIM, 1)
        value_head = lax.dynamic_slice_in_dim(values, kv_start, HEAD_DIM, 1)
        scores = jnp.dot(query_head, key_head.T, preferred_element_type=jnp.float32) * score_scale
        row_peak = lax.optimization_barrier(jnp.max(scores, axis=1))
        log_totals = row_peak + jnp.log(lax.optimization_barrier(jnp.sum(jnp.exp(scores - row_peak[:, None]), axis=1)))
        weights = jnp.exp(scores - log_totals[:, None])
        weights_rounded = weights.astype(jnp.bfloat16)
        grad_weights = jnp.dot(grad_head, value_head.T, preferred_element_type=jnp.float32)
        grad_scores = (weights * (grad_weights - delta_head[:, None]) * score_scale).astype(jnp.bfloat16)
        query_part = jnp.dot(grad_scores, key_head, preferred_element_type=jnp.float32)
        key_part = jnp.dot(grad_scores.T, query_head, preferred_element_type=jnp.float32)
        value_part = jnp.dot(weights_rounded.T, grad_head, preferred_element_type=jnp.float32)
        return (query_part, key_part, value_part)
    query_parts, key_parts, value_parts = lax.map(one_head, (query_heads, grad_heads, deltas, head_ids))
    query_grad = query_parts.astype(jnp.bfloat16).transpose(1, 0, 2).reshape(row_count, HEADS * HEAD_DIM)
    grad_keys = key_parts.reshape(KV_HEADS, group_size, source_count, HEAD_DIM).sum(axis=1)
    grad_keys = grad_keys.transpose(1, 0, 2).reshape(source_count, KV_HEADS * HEAD_DIM)
    grad_values = value_parts.reshape(KV_HEADS, group_size, source_count, HEAD_DIM).sum(axis=1)
    grad_values = grad_values.transpose(1, 0, 2).reshape(source_count, KV_HEADS * HEAD_DIM)
    grad_rows = jnp.dot(query_grad, w_query.T, preferred_element_type=jnp.float32).astype(jnp.bfloat16)
    grad_weight = jnp.dot(normed.T, query_grad, preferred_element_type=jnp.float32)
    return (grad_rows, grad_weight, grad_keys, grad_values)
```

```python
import functools
import math

import jax
import jax.numpy as jnp
from jax import lax
from jax.experimental import pallas as pl
from jax.experimental.pallas import tpu as pltpu
from jax.sharding import PartitionSpec as P

WIDTH = 4096
HEADS = 16
KV_HEADS = 4
HEAD_DIM = 256


norm_eps = 1e-06


def merged(part, axis, combine):
    gathered = jax.tree.map(lambda a: lax.all_gather(a, axis), part)

    def take(source):
        return jax.tree.map(lambda a: lax.dynamic_index_in_dim(a, source, 0, False), gathered)

    return lax.fori_loop(
        1, lax.axis_size(axis), lambda source, state: combine(state, take(source)), take(0)
    )


def join_stats(first_part, second_part):
    row_peak = jnp.maximum(first_part[0], second_part[0])
    summed = first_part[1] * jnp.exp(first_part[0] - row_peak) + second_part[1] * jnp.exp(
        second_part[0] - row_peak
    )
    return (row_peak, summed, first_part[2] + second_part[2])


def local(target, gain, w_query, queries, keys, values, attn_out, grad_out):
    local_heads = queries.shape[1] // HEAD_DIM
    group_size = HEADS // KV_HEADS
    score_scale = HEAD_DIM ** (-0.5)
    own_rows = queries.shape[0]
    src_rows = keys.shape[0]
    kv_index = lax.axis_index("tp") * local_heads // group_size
    key_own = lax.dynamic_slice_in_dim(keys, kv_index * HEAD_DIM, HEAD_DIM, 1)
    value_own = lax.dynamic_slice_in_dim(values, kv_index * HEAD_DIM, HEAD_DIM, 1)
    out_heads = attn_out.reshape(own_rows, local_heads, HEAD_DIM).astype(jnp.float32)
    grad_heads = grad_out.reshape(own_rows, local_heads, HEAD_DIM).astype(jnp.float32)
    delta_own = jnp.sum(out_heads * grad_heads, axis=2)
    empty_sum = jnp.zeros((src_rows, HEAD_DIM), jnp.float32)
    total_rows = own_rows * lax.axis_size("sp")
    position = lax.axis_index("sp") * own_rows
    delta_full = lax.dynamic_update_slice_in_dim(
        jnp.zeros((total_rows, local_heads), jnp.float32), delta_own, position, 0
    )
    query_all, grad_all = (
        lax.all_gather(queries, "sp", axis=0, tiled=True),
        lax.all_gather(grad_out, "sp", axis=0, tiled=True),
    )
    block_rows = math.gcd(total_rows, 512)
    block_count = total_rows // block_rows
    query_blocks = query_all.reshape(block_count, block_rows, local_heads, HEAD_DIM)
    grad_blocks = grad_all.reshape(block_count, block_rows, local_heads, HEAD_DIM)

    def block_stats(query_block):
        scores = (
            jnp.einsum("qhd,sd->hqs", query_block, key_own, preferred_element_type=jnp.float32)
            * score_scale
        )
        row_peak = jnp.max(scores, axis=2)
        row_total = jnp.sum(jnp.exp(scores - row_peak[:, :, None]), axis=2)
        return (row_peak, row_total)

    peaks, totals = lax.map(block_stats, query_blocks)
    peaks, totals, delta_full = merged((peaks, totals, delta_full), "sp", join_stats)
    log_totals = peaks + jnp.log(totals)
    delta_blocks = delta_full.reshape(block_count, block_rows, local_heads)

    def block_grads(running, inputs):
        query_block, grad_block, delta_block, log_block = inputs
        scores = (
            jnp.einsum("qhd,sd->hqs", query_block, key_own, preferred_element_type=jnp.float32)
            * score_scale
        )
        weights = jnp.exp(scores - log_block[:, :, None])
        grad_weights = jnp.einsum(
            "qhd,sd->hqs", grad_block, value_own, preferred_element_type=jnp.float32
        )
        delta_cols = jnp.transpose(delta_block)
        grad_scores = (weights * (grad_weights - delta_cols[:, :, None]) * score_scale).astype(
            jnp.bfloat16
        )
        key_sum = running[0] + jnp.einsum(
            "hqs,qhd->sd", grad_scores, query_block, preferred_element_type=jnp.float32
        )
        value_sum = running[1] + jnp.einsum(
            "hqs,qhd->sd",
            weights.astype(jnp.bfloat16),
            grad_block,
            preferred_element_type=jnp.float32,
        )
        query_part = jnp.einsum(
            "hqs,sd->qhd", grad_scores, key_own, preferred_element_type=jnp.float32
        )
        return ((key_sum, value_sum), query_part)

    (key_sum, value_sum), query_parts = lax.scan(
        block_grads, (empty_sum, empty_sum), (query_blocks, grad_blocks, delta_blocks, log_totals)
    )
    query_parts = query_parts.reshape(total_rows, 1, local_heads * HEAD_DIM)
    received = lax.all_to_all(
        query_parts.astype(jnp.bfloat16), "sp", split_axis=0, concat_axis=1, tiled=True
    ).astype(query_parts.dtype)
    query_grad = jnp.sum(received, axis=1)
    key_cols = key_sum.reshape(src_rows, 1, HEAD_DIM)
    value_cols = value_sum.reshape(src_rows, 1, HEAD_DIM)
    key_parts, value_parts = (
        lax.all_to_all(
            key_cols.astype(jnp.bfloat16), "tp", split_axis=0, concat_axis=1, tiled=True
        ).astype(key_cols.dtype),
        lax.all_to_all(
            value_cols.astype(jnp.bfloat16), "tp", split_axis=0, concat_axis=1, tiled=True
        ).astype(value_cols.dtype),
    )
    part_rows = key_parts.shape[0]
    per_kv = key_parts.shape[1] // KV_HEADS
    grad_keys = (
        key_parts.reshape(part_rows, KV_HEADS, per_kv, HEAD_DIM)
        .sum(axis=2)
        .reshape(part_rows, KV_HEADS * HEAD_DIM)
    )
    grad_values = (
        value_parts.reshape(part_rows, KV_HEADS, per_kv, HEAD_DIM)
        .sum(axis=2)
        .reshape(part_rows, KV_HEADS * HEAD_DIM)
    )
    query_grad = query_grad.astype(jnp.bfloat16)
    query_all_heads = lax.all_gather(query_grad, "tp", axis=1, tiled=True)
    grad_rows = lax.dot_general(
        query_all_heads, w_query, (((1,), (1,)), ((), ())), preferred_element_type=jnp.float32
    ).astype(jnp.bfloat16)
    target_wide = target.astype(jnp.float32)
    squares = lax.psum(jnp.sum(target_wide * target_wide, axis=1), "tp")
    inverse = lax.rsqrt(squares / WIDTH + norm_eps)
    normed = (target_wide * inverse[:, None] * gain).astype(jnp.bfloat16)
    grad_weight = lax.psum_scatter(
        lax.dot_general(
            normed, query_all_heads, (((0,), (0,)), ((), ())), preferred_element_type=jnp.float32
        ).astype(jnp.bfloat16),
        "sp",
        scatter_dimension=0,
        tiled=True,
    ).astype(jnp.float32)
    return (grad_rows, grad_weight, grad_keys, grad_values)


MESH = pl.DeviceIdType.MESH
BF16, F32 = jnp.bfloat16, jnp.float32
NT = (((1,), (1,)), ((), ()))
X = 2
ZS = 4
CHUNK = 256
NB = 2


def fused_kernel(
    ts, heads,
    target, gain, w_query, queries, keys, values, attn_out, grad_out,
    grad_rows, grad_weight, grad_keys, grad_values,
    qs, dos, outs, kbuf, vbuf, ktr, delta, sbuf, pbuf, dsbuf, qpart, part_in,
    stat, ksum, kv_out, kv_in, kv_tp, kv_tp_in, sq, ntr, nall,
    qown, qmate, qt, dqg, wbuf, res_out, res_in, send, recv, local_sem,
):
    rows = queries.shape[0]
    src = keys.shape[0]
    hd = HEAD_DIM
    width = heads * hd
    half = width // X
    cb = half // NB
    cols = heads * rows
    part = src // ts
    feat = target.shape[1] // (ZS * X)
    scale = hd ** (-0.5)
    sp, tp = lax.axis_index("sp"), lax.axis_index("tp")
    z, x = sp // X, sp % X
    core = tp % 2
    side = z // 2
    outer = 1 - (z + side) % 2
    inner = outer == 0
    z_mate, z_oin, z_oout = 1 + 4 * side - z, 2 - side, 3 - 3 * side
    sib = tp + 1 - 2 * core
    tps = [tp, sib, (tp + 2) % ts, (sib + 2) % ts]
    x_off = 1 - x
    slots_z = [z, z_mate, z_oin, z_oout]

    def dev(zz, xx, tt):
        return (zz * X + xx, tt)

    mate, oin, oout = (dev(a, x, tp) for a in (z_mate, z_oin, z_oout))
    xpeer = dev(z, x_off, tp)
    counts = {"send": 0, "recv": 0, "local": 0}
    pending = []

    def take(kind, n=1):
        at = counts[kind]
        counts[kind] += n
        return at

    def copy_of(source, dest, device, si, ri):
        return pltpu.make_async_remote_copy(
            src_ref=source, dst_ref=dest, send_sem=send.at[si], recv_sem=recv.at[ri],
            device_id=device, device_id_type=MESH,
        )

    def push(source, dest, device, ri, when=None):
        copy = copy_of(source, dest, device, take("send"), ri)
        if when is None:
            copy.start()
        else:
            pl.when(when)(copy.start)
        pending.append((copy, when))

    def arrived(view, ri):
        copy_of(view, view, xpeer, 0, ri).wait_recv()

    def fetch(source, dest):
        copy = pltpu.make_async_copy(source, dest, local_sem.at[take("local")])
        copy.start()
        return copy

    head_col = pl.ds(pl.multiple_of(tp * hd, hd), hd)
    loads = {}
    for name, ref, buf in (("q", queries, qs), ("d", grad_out, dos), ("o", attn_out, outs)):
        loads[name] = []
        for h in range(heads):
            view = buf.at[pl.ds(h * rows, rows)] if buf is outs else buf.at[0, pl.ds(h * rows, rows)]
            loads[name].append(fetch(ref.at[:, pl.ds(h * hd, hd)], view))
    k_load = fetch(keys.at[:, head_col], kbuf.at[pl.ds(0, src)])
    v_load = fetch(values.at[:, head_col], vbuf.at[pl.ds(0, src)])
    w_loads = [
        fetch(w_query.at[:, pl.ds(pl.multiple_of(t * width, width), width)], wbuf.at[e])
        for e, t in enumerate(tps)
    ]

    barrier = pltpu.get_barrier_semaphore()
    peers = [dev(a, x, tp) for a in slots_z[1:]] + [dev(a, x_off, tp) for a in slots_z]
    peers += [dev(z, xx, t) for xx in (x, x_off) for t in tps[1:]]
    for peer in peers:
        pl.semaphore_signal(barrier, inc=1, device_id=peer, device_id_type=MESH)

    wide = target[...].astype(F32)
    sq[0] = jnp.broadcast_to(jnp.sum(wide * wide, axis=1, keepdims=True), (rows, 128))
    for copy in loads["d"] + loads["o"]:
        copy.wait()
    for h in range(heads):
        span = pl.ds(h * rows, rows)
        dot = jnp.sum(dos[0, span].astype(F32) * outs[span].astype(F32), axis=1, keepdims=True)
        delta[0, :, span] = jnp.broadcast_to(dot, (rows, 128)).T[:1]
    for copy in [*loads["q"], k_load, v_load]:
        copy.wait()
    pl.semaphore_wait(barrier, len(peers))

    q_r, d_r, delta_r = take("recv", 4), take("recv", 4), take("recv", 4)
    k_r, v_r = take("recv"), take("recv")
    sq_r = take("recv", 4)

    def gather(buf, base, a, b, device, when=None):
        push(buf.at[a], buf.at[b], device, base + b, when)

    far = 2 + outer
    push(delta.at[0], delta.at[1], mate, delta_r + 1)
    push(delta.at[0], delta.at[far], oin, delta_r + far)
    push(delta.at[0], delta.at[far], oout, delta_r + far)
    for e in range(1, ts):
        push(sq.at[0], sq.at[e], dev(z, x, tps[e]), sq_r + e)
    gather(qs, q_r, 0, 1, mate)
    gather(qs, q_r, 0, 2, oin, inner)
    push(kbuf.at[pl.ds(0, src)], kbuf.at[pl.ds(src, src)], xpeer, k_r)
    gather(dos, d_r, 0, 1, mate)
    gather(dos, d_r, 0, 2, oin, inner)
    push(vbuf.at[pl.ds(0, src)], vbuf.at[pl.ds(src, src)], xpeer, v_r)

    ktr[:, :src] = kbuf[:src].T

    for e in range(1, ts):
        arrived(sq.at[e], sq_r + e)
    total = sq[0]
    for e in range(1, ts):
        total = total + sq[e]
    inverse = lax.rsqrt(total[:, :1] / (target.shape[1] * ts) + norm_eps)
    normed = target[...].astype(F32) * inverse * gain[...]
    ntr[...] = normed.T.astype(BF16)

    def feature_rows(zz, xx):
        return pl.ds(pl.multiple_of((zz * X + xx) * feat, feat), feat)

    def block(xx, t):
        return xx * ts + t

    def lanes(slot, xx):
        return pl.ds(pl.multiple_of((slot * X + xx) * rows, rows), rows)

    n_r = take("recv", ZS * X)
    own = block(x, tp)
    for xr, xx in enumerate((x, x_off)):
        for k, (zz, slot) in enumerate(((z_oin, far), (z_oout, far), (z_mate, 1), (z, 0))):
            if k == 3 and xr == 0:
                continue
            push(
                ntr.at[feature_rows(zz, xx)], nall.at[block(xx, tp), :, lanes(slot, x)],
                dev(zz, xx, tp), n_r + X * slot + xr,
            )
    nall[own, :, lanes(0, x)] = ntr[feature_rows(z, x)]

    def relay(buf, base, a, b, device):
        arrived(buf.at[a], base + a)
        gather(buf, base, a, b, device)

    def relay_inner(buf, base, a, b, device):
        copy = copy_of(buf.at[a], buf.at[b], device, take("send"), base + b)

        @pl.when(inner)
        def _():
            arrived(buf.at[a], base + a)
            copy.start()

        pending.append((copy, inner))

    def arrived_outer(buf, base, a):
        @pl.when(outer > 0)
        def _():
            arrived(buf.at[a], base + a)

    chunks = X * src // CHUNK

    def scores_of(j):
        def step(c, peak):
            span = pl.ds(pl.multiple_of(c * CHUNK, CHUNK), CHUNK)
            s = lax.dot_general(kbuf[span], qs[j], NT, preferred_element_type=F32)
            sbuf[span] = s
            return jnp.maximum(peak, jnp.max(s, axis=0, keepdims=True))

        return lax.fori_loop(0, chunks, step, jnp.full((1, cols), -jnp.inf, F32))

    def grads_of(j, peak):
        own_delta = delta[j]

        def step(c, total):
            span = pl.ds(pl.multiple_of(c * CHUNK, CHUNK), CHUNK)
            p = jnp.exp((sbuf[span] - peak) * scale)
            dp = lax.dot_general(vbuf[span], dos[j], NT, preferred_element_type=F32)
            pbuf[j, span] = p.astype(BF16)
            dsbuf[j, span] = (p * (dp - own_delta) * scale).astype(BF16)
            return total + jnp.sum(p, axis=0, keepdims=True)

        total = lax.fori_loop(0, chunks, step, jnp.zeros((1, cols), F32))
        stat[0, slots_z[j], 0:1] = peak * scale
        stat[0, slots_z[j], 1:2] = total
        qpart[j] = jnp.dot(ktr[...], dsbuf[j], preferred_element_type=F32).astype(BF16)

    stat_r, part_r = take("recv", ZS * ZS), take("recv", 6)

    def share(j):
        zt = slots_z[j]
        push(stat.at[0, zt], stat.at[far, zt], oin, stat_r + ZS * far + j)
        push(stat.at[0, zt], stat.at[1, zt], mate, stat_r + ZS + j)
        push(stat.at[0, zt], stat.at[far, zt], oout, stat_r + ZS * far + j)
        if j < 2:
            push(qpart.at[j], part_in.at[0, 1 - j], mate, part_r + 1 - j, outer > 0)
        else:
            i = far - 1
            push(qpart.at[j], part_in.at[i, j - 2], oin, part_r + 2 * i + j - 2)

    arrived(kbuf.at[pl.ds(src, src)], k_r)
    ktr[:, src:] = kbuf[src:].T
    arrived_outer(qs, q_r, 1)
    relay_inner(qs, q_r, 1, 3, oin)
    relay_inner(qs, q_r, 2, 2, mate)
    peak = scores_of(0)
    arrived_outer(dos, d_r, 1)
    relay_inner(dos, d_r, 1, 3, oin)
    relay_inner(dos, d_r, 2, 2, mate)
    arrived(vbuf.at[pl.ds(src, src)], v_r)
    grads_of(0, peak)
    share(0)
    arrived(delta.at[1], delta_r + 1)
    grads_of(1, scores_of(1))
    share(1)
    relay_inner(qs, q_r, 3, 3, mate)
    arrived_outer(qs, q_r, 2)
    for j in (2, 3):
        arrived(delta.at[j], delta_r + j)
    peak = scores_of(2)
    arrived_outer(dos, d_r, 2)
    grads_of(2, peak)
    share(2)
    relay_inner(dos, d_r, 3, 3, mate)
    for slot in range(ZS):
        for xr in range(X):
            if slot or xr:
                arrived(nall.at[0, :, pl.ds(0, rows)], n_r + X * slot + xr)
    n2_r, n3_r = take("recv", 4), take("recv", 4)
    places = [(x, tps[0]), (x_off, tps[0]), (x, tps[2]), (x_off, tps[2])]
    for i in (3, 1, 2):
        push(nall.at[own], nall.at[own], dev(z, *places[i]), n2_r + i)
    push(nall.at[own], nall.at[own], dev(z, x, sib), n3_r)
    arrived_outer(qs, q_r, 3)
    peak = scores_of(3)
    arrived_outer(dos, d_r, 3)
    grads_of(3, peak)
    share(3)

    def factors(j):
        zt = slots_z[j]
        tops = [stat[e, zt, 0:1] for e in range(ZS)]
        top = functools.reduce(jnp.maximum, tops)
        scaled = [jnp.exp(m - top) for m in tops]
        summed = sum(f * stat[e, zt, 1:2] for e, f in enumerate(scaled))
        return [f / summed for f in scaled]

    def reduced(j, out):
        f = factors(j)
        grad_t = qpart[j].astype(F32) * f[0]
        for i in range(3):
            arrived(part_in.at[i, j], part_r + 2 * i + j)
            grad_t = grad_t + part_in[i, j].astype(F32) * f[i + 1]
        grad_own = grad_t.T
        for h in range(heads):
            out[:, pl.ds(h * hd, hd)] = grad_own[h * rows : (h + 1) * rows].astype(BF16)

    xs_r = take("recv", 2 * NB)
    g_r = take("recv", ZS * NB)
    qt_r = take("recv", ts)
    own_r = take("recv")

    def rows_of(slot, xx):
        return pl.ds(pl.multiple_of((slot * X + xx) * rows, rows), rows)

    def g_view(b, slot):
        return dqg.at[b, pl.ds(slot * X * rows, X * rows)]

    def col_of(xx, b):
        return pl.ds(pl.multiple_of(xx * half + b * cb, cb), cb)

    def spread(slot, buf, when=None):
        for b in range(NB):
            push(
                buf.at[:, col_of(x_off, b)], dqg.at[b, rows_of(slot, x)], xpeer,
                xs_r + slot * NB + b, when,
            )

    def keep(slot, buf):
        for b in range(NB):
            dqg[b, rows_of(slot, x)] = buf[:, col_of(x, b)]

    def joined(slot, b):
        arrived(dqg.at[b, pl.ds(0, rows)], xs_r + slot * NB + b)

    def hand(slot, to, b, device):
        push(g_view(b, slot), g_view(b, to), device, g_r + ZS * b + to, inner)

    def came(slot, b):
        arrived(g_view(b, slot), g_r + ZS * b + slot)

    def qt_sends(when):
        push(qown, qt.at[2], dev(z, x, tps[2]), qt_r + 2, when)
        push(qown, qt.at[1], dev(z, x, sib), qt_r + 1, when)

    arrived(stat.at[1, 0], stat_r + ZS + 1)
    arrived(stat.at[2, 0], stat_r + ZS * 2 + 2)
    arrived(stat.at[3, 0], stat_r + ZS * 3 + 2)

    @pl.when(inner)
    def _():
        reduced(0, qown)
        keep(0, qown)

    spread(0, qown, inner)
    qt_sends(inner)
    for i in (1, 2, 3):
        xx, t = places[i]
        arrived(nall.at[0], n2_r + i)
        push(nall.at[block(xx, t)], nall.at[block(xx, t)], dev(z, x, sib), n3_r + i)
    for b in range(NB):
        @pl.when(inner)
        def _():
            joined(0, b)

        hand(0, 2, b, oin)
        hand(0, 1, b, mate)

    for e, js in ((1, (0, 2, 3)), (2, (0, 1, 3)), (3, (0, 1, 3))):
        for j in js:
            arrived(stat.at[e, 0], stat_r + ZS * e + j)

    @pl.when(inner)
    def _():
        reduced(1, qmate)

    push(qmate, qown, mate, own_r, inner)
    spread(1, qmate, inner)

    @pl.when(inner)
    def _():
        keep(1, qmate)

    for j in range(ZS):
        r = factors(j)[0]
        r = jnp.broadcast_to(r, (128, cols)).T
        r = jnp.concatenate([r] * (hd // 128), axis=1)
        q_scaled = (qs[j].astype(F32) * r).astype(BF16)
        d_scaled = (dos[j].astype(F32) * r).astype(BF16)
        for i, (left, right) in enumerate(((dsbuf, q_scaled), (pbuf, d_scaled))):
            piece = jnp.dot(left[j], right, preferred_element_type=F32)
            ksum[i] = piece if j == 0 else ksum[i] + piece
    kv_out[...] = ksum[:, src:].astype(BF16)
    kvx_r = take("recv")
    push(kv_out, kv_in, xpeer, kvx_r)

    def pass_on(slot, b):
        copy = copy_of(g_view(b, slot), g_view(b, slot), mate, take("send"), g_r + ZS * b + slot)

        @pl.when(inner)
        def _():
            came(slot, b)
            copy.start()

        pending.append((copy, inner))

    for b in range(NB):
        pass_on(2, b)

        @pl.when(inner)
        def _():
            joined(1, b)

        hand(1, 3, b, oin)
    @pl.when(outer > 0)
    def _():
        arrived(qown, own_r)
        keep(0, qown)

    spread(0, qown, outer > 0)
    qt_sends(outer > 0)

    arrived(kv_in, kvx_r)
    for i in range(2):
        ksum[i, :src] = ksum[i, :src] + kv_in[i].astype(F32)
    kv_tp[...] = ksum[:, :src].astype(BF16)

    def part_rows(t):
        return pl.ds(pl.multiple_of(t * part, part), part)

    kvt_r = take("recv", ts)
    for e in range(1, ts):
        push(kv_tp.at[:, part_rows(tps[e])], kv_tp_in.at[e], dev(z, x, tps[e]), kvt_r + e)
    for i, out in enumerate((grad_keys, grad_values)):
        out[:, head_col] = ksum[i, part_rows(tp)]

    w_loads[0].wait()
    rows_sum = lax.dot_general(qown[...], wbuf[0], NT, preferred_element_type=F32)
    arrived(qt.at[2], qt_r + 2)
    push(qt.at[2], qt.at[3], dev(z, x, sib), qt_r + 3)
    for i in range(4):
        arrived(nall.at[0], n3_r + i)

    res_r = take("recv", NB * X * ts)
    order = [(1, 3), (1, 2), (0, 3), (0, 2), (1, 1), (1, 0), (0, 1), (0, 0)]

    def project(b):
        for xr, e in order:
            xx, k = (x, x_off)[xr], xr * ts + e
            piece = jnp.dot(nall[block(xx, tps[e])], dqg[b], preferred_element_type=F32)
            if k:
                res_out[b, k] = piece.astype(BF16)
                push(
                    res_out.at[b, k], res_in.at[b, k], dev(z, xx, tps[e]),
                    res_r + b * X * ts + k,
                )
            else:
                at = pl.multiple_of(tp * width + x * half + b * cb, cb)
                grad_weight[:, pl.ds(at, cb)] = piece

    for b in range(NB):
        @pl.when(outer > 0)
        def _():
            joined(0, b)
            came(1, b)
            came(2, b)
            came(3, b)

        pass_on(3, b)
        project(b)

    for e in (1, 2, 3):
        if e != 2:
            arrived(qt.at[e], qt_r + e)
        w_loads[e].wait()
        rows_sum = rows_sum + lax.dot_general(qt[e], wbuf[e], NT, preferred_element_type=F32)
    grad_rows[...] = rows_sum.astype(BF16)
    for e in range(1, ts):
        arrived(kv_tp_in.at[e], kvt_r + e)
        at = pl.ds(pl.multiple_of(tps[e] * hd, hd), hd)
        for i, out in enumerate((grad_keys, grad_values)):
            out[:, at] = kv_tp_in[e, i].astype(F32)
    for b in range(NB):
        for xr, e in order[:-1]:
            xx, k = (x, x_off)[xr], xr * ts + e
            arrived(res_in.at[b, k], res_r + b * X * ts + k)
            at = pl.multiple_of(tps[e] * width + xx * half + b * cb, cb)
            grad_weight[:, pl.ds(at, cb)] = res_in[b, k].astype(F32)
    for copy, when in pending:
        if when is None:
            copy.wait_send()
        else:
            pl.when(when)(copy.wait_send)


def fused(target, gain, w_query, queries, keys, values, attn_out, grad_out):
    ts = lax.axis_size("tp")
    rows, width = queries.shape
    src = keys.shape[0]
    heads = width // HEAD_DIM
    cols, hd = heads * rows, HEAD_DIM
    feats = target.shape[1]
    feat = feats // (ZS * X)
    part = src // ts
    cb = width // X // NB
    vmem, hbm = pl.BlockSpec(memory_space=pltpu.VMEM), pl.BlockSpec(memory_space=pl.ANY)
    return pl.pallas_call(
        functools.partial(fused_kernel, ts, heads),
        out_shape=(
            jax.ShapeDtypeStruct((rows, feats), BF16),
            jax.ShapeDtypeStruct((feat, width * ts), F32),
            jax.ShapeDtypeStruct((part, keys.shape[1]), F32),
            jax.ShapeDtypeStruct((part, keys.shape[1]), F32),
        ),
        in_specs=[vmem, vmem, hbm, hbm, hbm, hbm, hbm, hbm],
        out_specs=(vmem,) * 4,
        scratch_shapes=[
            pltpu.VMEM((ZS, cols, hd), BF16),
            pltpu.VMEM((ZS, cols, hd), BF16),
            pltpu.VMEM((cols, hd), BF16),
            pltpu.VMEM((X * src, hd), BF16),
            pltpu.VMEM((X * src, hd), BF16),
            pltpu.VMEM((hd, X * src), BF16),
            pltpu.VMEM((ZS, 1, cols), F32),
            pltpu.VMEM((X * src, cols), F32),
            pltpu.VMEM((ZS, X * src, cols), BF16),
            pltpu.VMEM((ZS, X * src, cols), BF16),
            pltpu.VMEM((ZS, hd, cols), BF16),
            pltpu.VMEM((3, 2, hd, cols), BF16),
            pltpu.VMEM((ZS, ZS, 2, cols), F32),
            pltpu.VMEM((2, X * src, hd), F32),
            pltpu.VMEM((2, src, hd), BF16),
            pltpu.VMEM((2, src, hd), BF16),
            pltpu.VMEM((2, src, hd), BF16),
            pltpu.VMEM((ts, 2, part, hd), BF16),
            pltpu.VMEM((ts, rows, 128), F32),
            pltpu.VMEM((feats, rows), BF16),
            pltpu.VMEM((X * ts, feat, ZS * X * rows), BF16),
            pltpu.VMEM((rows, width), BF16),
            pltpu.VMEM((rows, width), BF16),
            pltpu.VMEM((ts, rows, width), BF16),
            pltpu.VMEM((NB, ZS * X * rows, cb), BF16),
            pltpu.VMEM((ts, feats, width), BF16),
            pltpu.VMEM((NB, X * ts, feat, cb), BF16),
            pltpu.VMEM((NB, X * ts, feat, cb), BF16),
            pltpu.SemaphoreType.DMA((96 + 24 * NB,)),
            pltpu.SemaphoreType.DMA((80 + 14 * NB,)),
            pltpu.SemaphoreType.DMA((2 + 3 * heads + ts,)),
        ],
        compiler_params=pltpu.CompilerParams(
            collective_id=0, has_side_effects=True, vmem_limit_bytes=60 * 2**20
        ),
    )(target, gain.reshape(1, feats), w_query, queries, keys, values, attn_out, grad_out)


def fits(mesh):
    sp, tp = mesh.shape["sp"], mesh.shape["tp"]
    feat = WIDTH // (sp * tp)
    return tp == KV_HEADS and sp == ZS * X and feat % 128 == 0


def solution(mesh):
    return jax.shard_map(
        fused if fits(mesh) else local,
        mesh=mesh,
        in_specs=(
            P("sp", "tp"),
            P("tp"),
            P("tp", None),
            P("sp", "tp"),
            P("sp", None),
            P("sp", None),
            P("sp", "tp"),
            P("sp", "tp"),
        ),
        out_specs=(
            P("sp", "tp"),
            P(("tp", "sp"), None),
            P(("sp", "tp"), None),
            P(("sp", "tp"), None),
        ),
        check_vma=False,
    )
```

```python
import functools
import math

import jax
import jax.numpy as jnp
from jax import lax
from jax.experimental import pallas as pl
from jax.experimental.pallas import tpu as pltpu
from jax.sharding import PartitionSpec as P

WIDTH = 4096
HEADS = 16
KV_HEADS = 4
HEAD_DIM = 256


norm_eps = 1e-06


def merged(part, axis, combine):
    gathered = jax.tree.map(lambda a: lax.all_gather(a, axis), part)

    def take(source):
        return jax.tree.map(lambda a: lax.dynamic_index_in_dim(a, source, 0, False), gathered)

    return lax.fori_loop(
        1, lax.axis_size(axis), lambda source, state: combine(state, take(source)), take(0)
    )


def join_stats(first_part, second_part):
    row_peak = jnp.maximum(first_part[0], second_part[0])
    summed = first_part[1] * jnp.exp(first_part[0] - row_peak) + second_part[1] * jnp.exp(
        second_part[0] - row_peak
    )
    return (row_peak, summed, first_part[2] + second_part[2])


def local(target, gain, w_query, queries, keys, values, attn_out, grad_out):
    local_heads = queries.shape[1] // HEAD_DIM
    group_size = HEADS // KV_HEADS
    score_scale = HEAD_DIM ** (-0.5)
    own_rows = queries.shape[0]
    src_rows = keys.shape[0]
    kv_index = lax.axis_index("tp") * local_heads // group_size
    key_own = lax.dynamic_slice_in_dim(keys, kv_index * HEAD_DIM, HEAD_DIM, 1)
    value_own = lax.dynamic_slice_in_dim(values, kv_index * HEAD_DIM, HEAD_DIM, 1)
    out_heads = attn_out.reshape(own_rows, local_heads, HEAD_DIM).astype(jnp.float32)
    grad_heads = grad_out.reshape(own_rows, local_heads, HEAD_DIM).astype(jnp.float32)
    delta_own = jnp.sum(out_heads * grad_heads, axis=2)
    empty_sum = jnp.zeros((src_rows, HEAD_DIM), jnp.float32)
    total_rows = own_rows * lax.axis_size("sp")
    position = lax.axis_index("sp") * own_rows
    delta_full = lax.dynamic_update_slice_in_dim(
        jnp.zeros((total_rows, local_heads), jnp.float32), delta_own, position, 0
    )
    query_all, grad_all = (
        lax.all_gather(queries, "sp", axis=0, tiled=True),
        lax.all_gather(grad_out, "sp", axis=0, tiled=True),
    )
    block_rows = math.gcd(total_rows, 512)
    block_count = total_rows // block_rows
    query_blocks = query_all.reshape(block_count, block_rows, local_heads, HEAD_DIM)
    grad_blocks = grad_all.reshape(block_count, block_rows, local_heads, HEAD_DIM)

    def block_stats(query_block):
        scores = (
            jnp.einsum("qhd,sd->hqs", query_block, key_own, preferred_element_type=jnp.float32)
            * score_scale
        )
        row_peak = jnp.max(scores, axis=2)
        row_total = jnp.sum(jnp.exp(scores - row_peak[:, :, None]), axis=2)
        return (row_peak, row_total)

    peaks, totals = lax.map(block_stats, query_blocks)
    peaks, totals, delta_full = merged((peaks, totals, delta_full), "sp", join_stats)
    log_totals = peaks + jnp.log(totals)
    delta_blocks = delta_full.reshape(block_count, block_rows, local_heads)

    def block_grads(running, inputs):
        query_block, grad_block, delta_block, log_block = inputs
        scores = (
            jnp.einsum("qhd,sd->hqs", query_block, key_own, preferred_element_type=jnp.float32)
            * score_scale
        )
        weights = jnp.exp(scores - log_block[:, :, None])
        grad_weights = jnp.einsum(
            "qhd,sd->hqs", grad_block, value_own, preferred_element_type=jnp.float32
        )
        delta_cols = jnp.transpose(delta_block)
        grad_scores = (weights * (grad_weights - delta_cols[:, :, None]) * score_scale).astype(
            jnp.bfloat16
        )
        key_sum = running[0] + jnp.einsum(
            "hqs,qhd->sd", grad_scores, query_block, preferred_element_type=jnp.float32
        )
        value_sum = running[1] + jnp.einsum(
            "hqs,qhd->sd",
            weights.astype(jnp.bfloat16),
            grad_block,
            preferred_element_type=jnp.float32,
        )
        query_part = jnp.einsum(
            "hqs,sd->qhd", grad_scores, key_own, preferred_element_type=jnp.float32
        )
        return ((key_sum, value_sum), query_part)

    (key_sum, value_sum), query_parts = lax.scan(
        block_grads, (empty_sum, empty_sum), (query_blocks, grad_blocks, delta_blocks, log_totals)
    )
    query_parts = query_parts.reshape(total_rows, 1, local_heads * HEAD_DIM)
    received = lax.all_to_all(
        query_parts.astype(jnp.bfloat16), "sp", split_axis=0, concat_axis=1, tiled=True
    ).astype(query_parts.dtype)
    query_grad = jnp.sum(received, axis=1)
    key_cols = key_sum.reshape(src_rows, 1, HEAD_DIM)
    value_cols = value_sum.reshape(src_rows, 1, HEAD_DIM)
    key_parts, value_parts = (
        lax.all_to_all(
            key_cols.astype(jnp.bfloat16), "tp", split_axis=0, concat_axis=1, tiled=True
        ).astype(key_cols.dtype),
        lax.all_to_all(
            value_cols.astype(jnp.bfloat16), "tp", split_axis=0, concat_axis=1, tiled=True
        ).astype(value_cols.dtype),
    )
    part_rows = key_parts.shape[0]
    per_kv = key_parts.shape[1] // KV_HEADS
    grad_keys = (
        key_parts.reshape(part_rows, KV_HEADS, per_kv, HEAD_DIM)
        .sum(axis=2)
        .reshape(part_rows, KV_HEADS * HEAD_DIM)
    )
    grad_values = (
        value_parts.reshape(part_rows, KV_HEADS, per_kv, HEAD_DIM)
        .sum(axis=2)
        .reshape(part_rows, KV_HEADS * HEAD_DIM)
    )
    query_grad = query_grad.astype(jnp.bfloat16)
    query_all_heads = lax.all_gather(query_grad, "tp", axis=1, tiled=True)
    grad_rows = lax.dot_general(
        query_all_heads, w_query, (((1,), (1,)), ((), ())), preferred_element_type=jnp.float32
    ).astype(jnp.bfloat16)
    target_wide = target.astype(jnp.float32)
    squares = lax.psum(jnp.sum(target_wide * target_wide, axis=1), "tp")
    inverse = lax.rsqrt(squares / WIDTH + norm_eps)
    normed = (target_wide * inverse[:, None] * gain).astype(jnp.bfloat16)
    grad_weight = lax.psum_scatter(
        lax.dot_general(
            normed, query_all_heads, (((0,), (0,)), ((), ())), preferred_element_type=jnp.float32
        ).astype(jnp.bfloat16),
        "sp",
        scatter_dimension=0,
        tiled=True,
    ).astype(jnp.float32)
    return (grad_rows, grad_weight, grad_keys, grad_values)


MESH = pl.DeviceIdType.MESH
BF16, F32 = jnp.bfloat16, jnp.float32
NT = (((1,), (1,)), ((), ()))
X = 2
ZS = 4
CHUNK = 512
PIECES = 4


def fused_kernel(
    ts, heads,
    target, gain, w_query, queries, keys, values, attn_out, grad_out,
    rows_raw, weight_raw, kv_raw,
    qs, dos, outs, kbuf, vbuf, ktr, delta, sbuf, pbuf, dsbuf, qpart, part_in,
    side_out, side_in, stat, ksum, kv_out, kv_in, kv_tp, sq, ntr, nall,
    dqrow, qt, dqg, wbuf, res_out, rows_out, send, recv, local_sem,
):
    rows = queries.shape[0]
    src = keys.shape[0]
    hd = HEAD_DIM
    width = heads * hd
    groups = heads // X
    half = width // X
    gcols = X * rows
    part = src // ts
    feat = target.shape[1] // (ZS * X)
    scale = hd ** (-0.5)
    sp, tp = lax.axis_index("sp"), lax.axis_index("tp")
    z, x = sp // X, sp % X
    core = tp % 2
    side = z // 2
    outer = 1 - (z + side) % 2
    inner = outer == 0
    edge = outer > 0
    z_mate, z_oin, z_oout = 1 + 4 * side - z, 2 - side, 3 - 3 * side
    sib = tp + 1 - 2 * core
    tps = [tp, sib, (tp + 2) % ts, (sib + 2) % ts]
    x_off = 1 - x
    slots_z = [z, z_mate, z_oin, z_oout]
    swap = (1, 0, 2, 3)
    far = 2 + outer

    def dev(zz, xx, tt):
        return (zz * X + xx, tt)

    mate, oin, oout = (dev(a, x, tp) for a in (z_mate, z_oin, z_oout))
    xpeer, y_peer, sib_peer = dev(z, x_off, tp), dev(z, x, tps[2]), dev(z, x, sib)
    counts = {"send": 0, "recv": 0, "local": 0}
    pending = []

    def take(kind, n=1):
        at = counts[kind]
        counts[kind] += n
        return at

    def copy_of(source, dest, device, si, ri):
        return pltpu.make_async_remote_copy(
            src_ref=source, dst_ref=dest, send_sem=send.at[si], recv_sem=recv.at[ri],
            device_id=device, device_id_type=MESH,
        )

    def push(source, dest, device, ri, when=None):
        copy = copy_of(source, dest, device, take("send"), ri)
        if when is None:
            copy.start()
        else:
            pl.when(when)(copy.start)
        pending.append((copy, when))

    def arrived(view, ri):
        copy_of(view, view, xpeer, 0, ri).wait_recv()

    def fetch(source, dest):
        copy = pltpu.make_async_copy(source, dest, local_sem.at[take("local")])
        copy.start()
        return copy

    def head_of(g, xx):
        return xx * groups + g

    head_col = pl.ds(pl.multiple_of(tp * hd, hd), hd)
    loads = {"q": [], "d": [], "o": []}
    for name, ref, buf in (("q", queries, qs), ("d", grad_out, dos), ("o", attn_out, outs)):
        for g in range(groups):
            for xx in range(X):
                view = buf.at[g] if buf is outs else buf.at[g, 0]
                view = view.at[pl.ds(xx * rows, rows)]
                loads[name].append(fetch(ref.at[:, pl.ds(head_of(g, xx) * hd, hd)], view))
    k_load = fetch(keys.at[:, head_col], kbuf.at[pl.ds(0, src)])
    v_load = fetch(values.at[:, head_col], vbuf.at[pl.ds(0, src)])
    w_loads = [
        fetch(w_query.at[:, pl.ds(pl.multiple_of(t * width, width), width)], wbuf.at[e])
        for e, t in enumerate(tps)
    ]

    barrier = pltpu.get_barrier_semaphore()
    peers = [dev(a, x, tp) for a in slots_z[1:]] + [dev(a, x_off, tp) for a in slots_z]
    peers += [dev(z, xx, t) for xx in (x, x_off) for t in tps[1:]]
    for peer in peers:
        pl.semaphore_signal(barrier, inc=1, device_id=peer, device_id_type=MESH)

    wide = target[...].astype(F32)
    sq[0] = jnp.broadcast_to(jnp.sum(wide * wide, axis=1, keepdims=True), (rows, 128))
    for copy in loads["d"] + loads["o"]:
        copy.wait()
    for g in range(groups):
        dot = jnp.sum(dos[g, 0].astype(F32) * outs[g].astype(F32), axis=1, keepdims=True)
        delta[0, g] = jnp.broadcast_to(dot, (gcols, 128)).T[:1]
    for copy in [*loads["q"], k_load, v_load]:
        copy.wait()
    pl.semaphore_wait(barrier, len(peers))

    q_r, d_r = take("recv", ZS * groups), take("recv", ZS * groups)
    delta_r, sq_r = take("recv", ZS), take("recv", ZS)
    k_r, v_r = take("recv"), take("recv")

    def gather(buf, base, g, a, b, device, when=None):
        push(buf.at[g, a], buf.at[g, b], device, base + ZS * g + b, when)

    push(delta.at[0], delta.at[1], mate, delta_r + 1)
    push(delta.at[0], delta.at[far], oin, delta_r + far)
    push(delta.at[0], delta.at[far], oout, delta_r + far)
    for e in range(1, ts):
        push(sq.at[0], sq.at[e], dev(z, x, tps[e]), sq_r + e)
    gather(qs, q_r, 0, 0, 1, mate)
    gather(qs, q_r, 0, 0, 2, oin, inner)
    push(kbuf.at[pl.ds(0, src)], kbuf.at[pl.ds(src, src)], xpeer, k_r)
    gather(dos, d_r, 0, 0, 1, mate)
    gather(dos, d_r, 0, 0, 2, oin, inner)
    push(vbuf.at[pl.ds(0, src)], vbuf.at[pl.ds(src, src)], xpeer, v_r)
    for g in range(1, groups):
        gather(qs, q_r, g, 0, 1, mate)
        gather(dos, d_r, g, 0, 1, mate)

    ktr[:, :src] = kbuf[:src].T
    for e in range(1, ts):
        arrived(sq.at[e], sq_r + e)
    total = sq[0]
    for e in range(1, ts):
        total = total + sq[e]
    inverse = lax.rsqrt(total[:, :1] / (target.shape[1] * ts) + norm_eps)
    normed = target[...].astype(F32) * inverse * gain[...]
    ntr[...] = normed.T.astype(BF16)

    def feature_rows(zz, xx):
        return pl.ds(pl.multiple_of((zz * X + xx) * feat, feat), feat)

    def lanes(slot, xx):
        return pl.ds(pl.multiple_of((slot * X + xx) * rows, rows), rows)

    n_r = take("recv", ZS * X)
    n_in = take("recv", X * ts)

    def n_send(zz, slot, xr):
        xx = (x, x_off)[xr]
        push(
            ntr.at[feature_rows(zz, xx)], nall.at[0, :, lanes(slot, x)], dev(zz, xx, tp),
            n_r + X * slot + xr,
        )

    def n_pass(i, to, device, when=None):
        push(nall.at[i], nall.at[to], device, n_in + to, when)

    def n_relay(when):
        @pl.when(when)
        def _():
            arrived(nall.at[0], n_in + ts)

        n_pass(ts, ts + 2, y_peer, when)
        n_pass(ts, ts + 1, sib_peer, when)

    nall[0, :, lanes(0, x)] = ntr[feature_rows(z, x)]

    def relay(g, a, b, device):
        for buf, base in ((qs, q_r), (dos, d_r)):
            copy = copy_of(
                buf.at[g, a], buf.at[g, b], device, take("send"), base + ZS * g + b
            )

            @pl.when(inner)
            def _():
                arrived(buf.at[g, a], base + ZS * g + a)
                copy.start()

            pending.append((copy, inner))

    def gathered(g, a):
        @pl.when(edge)
        def _():
            arrived(qs.at[g, a], q_r + ZS * g + a)
            arrived(dos.at[g, a], d_r + ZS * g + a)

    chunks = X * src // CHUNK

    def scores_of(g, j):
        def step(c, peak):
            span = pl.ds(pl.multiple_of(c * CHUNK, CHUNK), CHUNK)
            s = lax.dot_general(kbuf[span], qs[g, j], NT, preferred_element_type=F32)
            sbuf[span] = s
            return jnp.maximum(peak, jnp.max(s, axis=0, keepdims=True))

        return lax.fori_loop(0, chunks, step, jnp.full((1, gcols), -jnp.inf, F32), unroll=True)

    def grads_of(g, j, peak):
        own_delta = delta[j, g]
        lane_span = pl.ds((g * ZS + j) * gcols, gcols)

        def step(c, total):
            span = pl.ds(pl.multiple_of(c * CHUNK, CHUNK), CHUNK)
            p = jnp.exp((sbuf[span] - peak) * scale)
            dp = lax.dot_general(vbuf[span], dos[g, j], NT, preferred_element_type=F32)
            pbuf[span, lane_span] = p.astype(BF16)
            dsbuf[span, lane_span] = (p * (dp - own_delta) * scale).astype(BF16)
            return total + jnp.sum(p, axis=0, keepdims=True)

        total = lax.fori_loop(0, chunks, step, jnp.zeros((1, gcols), F32), unroll=True)
        stat[0, slots_z[j], g, 0:1] = peak * scale
        stat[0, slots_z[j], g, 1:2] = total
        qpart[g, j] = jnp.dot(ktr[...], dsbuf[:, lane_span], preferred_element_type=F32).astype(BF16)

    stat_r = take("recv", groups * ZS * ZS)
    part_r, side_r = take("recv", groups * ZS), take("recv", groups * ZS)

    def stat_at(g, e, j):
        return stat_r + ZS * ZS * g + ZS * e + j

    def share(g, j):
        zt = slots_z[j]
        for e, device in ((far, oin), (far, oout), (1, mate)):
            push(stat.at[0, zt, g], stat.at[e, zt, g], device, stat_at(g, e, j))
        to = swap[j]
        push(qpart.at[g, j], part_in.at[g, to], mate, part_r + ZS * g + to, edge)

    def process(g, j):
        grads_of(g, j, scores_of(g, j))
        share(g, j)

    def weights_of(g, j, sources):
        zt = slots_z[j]
        tops = [stat[e, zt, g, 0:1] for e in sources]
        top = functools.reduce(jnp.maximum, tops)
        scaled = [jnp.exp(m - top) for m in tops]
        summed = sum(f * stat[e, zt, g, 1:2] for e, f in zip(sources, scaled))
        return top, scaled, summed

    def stats_came(g, j):
        there = (j + 2) % ZS
        for e, k in ((2, there), (3, there if there > 1 else swap[there])):
            arrived(stat.at[0, 0, 0], stat_at(g, e, k))

    def side_sum(g, j):
        @pl.when(inner)
        def _():
            arrived(stat.at[0, 0, 0], stat_at(g, 1, swap[j]))
            arrived(part_in.at[g, j], part_r + ZS * g + j)
            _, (f_own, f_mate), _ = weights_of(g, j, (0, 1))
            near_part = qpart[g, j].astype(F32) * f_own + part_in[g, j].astype(F32) * f_mate
            side_out[g, j] = near_part.astype(BF16)

        to = (j + 2) % ZS
        push(side_out.at[g, j], side_in.at[g, to], oin, side_r + ZS * g + to, inner)

    row_r, xs_r, g_r = (take("recv", groups * ZS) for _ in range(3))
    qt_r = take("recv", ts * groups)

    def rows_of(slot, xx):
        return pl.ds(pl.multiple_of((slot * X + xx) * rows, rows), rows)

    def lanes_of(xx):
        return pl.ds(pl.multiple_of(xx * hd, hd), hd)

    def spread(g, j, when):
        push(
            dqrow.at[g, j, :, lanes_of(x_off)], dqg.at[g, rows_of(j, x)], xpeer,
            xs_r + ZS * g + j, when,
        )

        @pl.when(when)
        def _():
            dqg[g, rows_of(j, x)] = dqrow[g, j, :, lanes_of(x)]

    def qt_sends(g, when):
        push(dqrow.at[g, 0], qt.at[2, g], y_peer, qt_r + groups * 2 + g, when)
        push(dqrow.at[g, 0], qt.at[1, g], sib_peer, qt_r + groups + g, when)

    def reduce_rows(g, j):
        @pl.when(inner)
        def _():
            arrived(side_in.at[g, j], side_r + ZS * g + j)
            top, _, summed = weights_of(g, j, range(ZS))
            near_top, far_top = (weights_of(g, j, pair)[0] for pair in ((0, 1), (2, 3)))
            grad_t = side_out[g, j].astype(F32) * (jnp.exp(near_top - top) / summed)
            grad_t = grad_t + side_in[g, j].astype(F32) * (jnp.exp(far_top - top) / summed)
            grad_own = grad_t.T.astype(BF16)
            for xx in range(X):
                dqrow[g, j, :, pl.ds(xx * hd, hd)] = grad_own[xx * rows : (xx + 1) * rows]

        spread(g, j, inner)
        if j == 0:
            qt_sends(g, inner)

    def joined(g, j):
        arrived(dqg.at[g, pl.ds(0, rows)], xs_r + ZS * g + j)

    def block_of(g, j):
        return dqg.at[g, pl.ds(j * X * rows, X * rows)]

    def hand(g, j):
        @pl.when(inner)
        def _():
            joined(g, j)

        push(block_of(g, j), block_of(g, swap[j]), mate, g_r + ZS * g + swap[j], inner)
        if j == 1:
            push(
                dqrow.at[g, 1, :, lanes_of(x_off)], dqrow.at[g, 0, :, lanes_of(x_off)], mate,
                row_r + g, inner,
            )

    def dkv():
        pairs = [(g, j) for g in range(groups) for j in range(ZS)]

        def stacked(e, i):
            rows_in = [stat[e, slots_z[j], g, i : i + 1] for g, j in pairs]
            return jnp.concatenate(rows_in, axis=0)

        tops = [stacked(e, 0) for e in range(ZS)]
        top = functools.reduce(jnp.maximum, tops)
        scaled = [jnp.exp(m - top) for m in tops]
        summed = sum(f * stacked(e, 1) for e, f in enumerate(scaled))
        ratios = (scaled[0] / summed).T
        for n in range(0, len(pairs), 2):
            held = []
            for i, buf in enumerate((qs, dos)):
                pieces = [
                    (buf[g, j].astype(F32) * ratios[:, n + k : n + k + 1]).astype(BF16)
                    for k, (g, j) in enumerate(pairs[n : n + 2])
                ]
                held.append(jnp.concatenate(pieces, axis=0))
            span = pl.ds(n * gcols, 2 * gcols)
            for i, left in enumerate((dsbuf, pbuf)):
                piece = jnp.dot(left[:, span], held[i], preferred_element_type=F32)
                ksum[i] = piece if n == 0 else ksum[i] + piece

    kvx_r, kvt_r = take("recv", 8), take("recv", ts)
    quarter = src // 4
    stores = []

    def kvx(first, last, when):
        for n in range(first, last):
            piece = pl.ds(n % 4 * quarter, quarter)
            push(kv_out.at[n // 4, piece], kv_in.at[n // 4, piece], xpeer, kvx_r + n, when)

    def part_rows(t):
        return pl.ds(pl.multiple_of(t * part, part), part)

    def kv_finish(when):
        @pl.when(when)
        def _():
            for n in range(8):
                arrived(kv_in.at[0, pl.ds(0, quarter)], kvx_r + n)
            for i in range(2):
                kv_tp[i] = (ksum[i, :src] + kv_in[i].astype(F32)).astype(BF16)

        for e in range(1, ts):
            push(
                kv_tp.at[:, part_rows(tps[e])], kv_raw.at[:, :, head_col], dev(z, x, tps[e]),
                kvt_r + e, when,
            )

    res_r = take("recv", groups * X * ts)
    order = [(xr, e) for xr in (1, 0) for e in (3, 2, 1, 0)]

    def res_push(g, xr, e, when=None):
        k = xr * ts + e
        at = pl.ds(pl.multiple_of(tp * width + x * half + g * hd, hd), hd)
        if k:
            push(
                res_out.at[g, k], weight_raw.at[:, at], dev(z, (x, x_off)[xr], tps[e]),
                res_r + g * X * ts + k, when,
            )
        else:
            stores.append(fetch(res_out.at[g, 0], weight_raw.at[:, at]))

    def project(g):
        for xr in (1, 0):
            block = nall[pl.ds(xr * ts, ts)].reshape(ts * feat, ZS * X * rows)
            result = jnp.dot(block, dqg[g], preferred_element_type=F32).astype(BF16)
            for e in range(ts):
                res_out[g, xr * ts + e] = result[e * feat : (e + 1) * feat]

    def ready(g):
        @pl.when(edge)
        def _():
            for j in (2, 3, 1, 0):
                arrived(block_of(g, j), g_r + ZS * g + j)

    def own_rows(g):
        @pl.when(edge)
        def _():
            dqrow[g, 0, :, lanes_of(x)] = dqg[g, rows_of(0, x)]
            arrived(dqrow.at[g, 0, :, pl.ds(0, hd)], row_r + g)

        qt_sends(g, edge)

    def qt_pass(g):
        arrived(qt.at[2, g], qt_r + groups * 2 + g)
        push(qt.at[2, g], qt.at[3, g], sib_peer, qt_r + groups * 3 + g)

    def rows_part(e, g):
        left = dqrow[g, 0] if e == 0 else qt[e, g]
        total = 0.0
        for xx in range(X):
            w_cols = wbuf[e, :, pl.ds(head_of(g, xx) * hd, hd)]
            total = total + lax.dot_general(
                left[:, xx * hd : (xx + 1) * hd], w_cols, NT, preferred_element_type=F32
            )
        return total

    relay(0, 1, 3, oin)
    relay(0, 2, 2, mate)
    for g in range(1, groups):
        gather(qs, q_r, g, 0, 2, oin, inner)
        gather(dos, d_r, g, 0, 2, oin, inner)
    arrived(kbuf.at[pl.ds(src, src)], k_r)
    ktr[:, src:] = kbuf[src:].T
    peak = scores_of(0, 0)
    arrived(vbuf.at[pl.ds(src, src)], v_r)
    relay(1, 1, 3, oin)
    grads_of(0, 0, peak)
    share(0, 0)
    relay(0, 3, 3, mate)
    for j in range(1, ZS):
        arrived(delta.at[j], delta_r + j)
    gathered(0, 1)
    process(0, 1)
    for xr in range(X):
        n_send(z_oin, far, xr)
        n_send(z_oout, far, xr)
        n_send(z_mate, 1, xr)
    n_send(z, 0, 1)
    relay(1, 2, 2, mate)
    gathered(0, 2)
    process(0, 2)
    gathered(0, 3)
    process(0, 3)
    side_sum(0, 0)
    side_sum(0, 1)
    relay(1, 3, 3, mate)
    gathered(1, 1)
    side_sum(0, 2)
    for slot in range(ZS):
        for xr in range(X):
            if slot or xr:
                arrived(nall.at[0, :, pl.ds(0, rows)], n_r + X * slot + xr)
    n_pass(0, ts, xpeer)
    n_pass(0, 2, y_peer)
    n_pass(0, 1, sib_peer)
    process(1, 0)
    process(1, 1)
    side_sum(0, 3)
    gathered(1, 2)
    process(1, 2)
    n_relay(edge)
    gathered(1, 3)
    process(1, 3)
    @pl.when(inner)
    def _():
        for j in range(ZS):
            stats_came(0, j)

    reduce_rows(0, 2)
    reduce_rows(0, 3)
    hand(0, 2)
    n_relay(inner)
    reduce_rows(0, 0)
    hand(0, 3)
    side_sum(1, 0)
    side_sum(1, 1)
    reduce_rows(0, 1)
    hand(0, 0)
    side_sum(1, 2)
    hand(0, 1)
    side_sum(1, 3)
    arrived(nall.at[0], n_in + 2)
    n_pass(2, 3, sib_peer)
    arrived(nall.at[0], n_in + ts + 2)
    n_pass(ts + 2, ts + 3, sib_peer)
    @pl.when(edge)
    def _():
        for g in range(groups):
            for e in range(1, ZS):
                for j in range(ZS):
                    arrived(stat.at[0, 0, 0], stat_at(g, e, j))

    @pl.when(inner)
    def _():
        for j in range(ZS):
            stats_came(1, j)

    reduce_rows(1, 2)
    reduce_rows(1, 3)
    @pl.when(inner)
    def _():
        for i in (1, 3, ts + 1, ts + 3):
            arrived(nall.at[0], n_in + i)

        project(0)

    for e in (3, 2):
        res_push(0, 1, e, inner)
    dkv()
    kv_out[...] = ksum[:, src:].astype(BF16)
    kvx(0, 8, edge)
    hand(1, 2)
    reduce_rows(1, 0)
    hand(1, 3)
    kvx(0, 1, inner)
    for e in (3, 2, 1):
        res_push(0, 0, e, inner)
    @pl.when(edge)
    def _():
        for i in (1, 3, ts + 1, ts + 3):
            arrived(nall.at[0], n_in + i)

    ready(0)
    @pl.when(edge)
    def _():
        project(0)

    for xr in (1, 0):
        for e in (3, 2, 1, 0):
            if xr or e:
                res_push(0, xr, e, edge)
    res_push(0, 0, 0)
    own_rows(0)
    hand(1, 0)
    reduce_rows(1, 1)
    kvx(1, 8, inner)
    hand(1, 1)
    for e in (1, 0):
        res_push(0, 1, e, inner)
    qt_pass(0)
    ready(1)
    project(1)
    for xr in (1, 0):
        for e in (3, 2, 1, 0):
            res_push(1, xr, e)
    own_rows(1)
    kv_finish(edge)
    kv_finish(inner)
    stores.append(fetch(kv_tp.at[:, part_rows(tp)], kv_raw.at[:, :, head_col]))
    for copy in w_loads:
        copy.wait()
    rows_sum = rows_part(0, 0) + rows_part(0, 1) + rows_part(2, 0)
    for e in (1, 3):
        arrived(qt.at[e, 0], qt_r + groups * e)
        rows_sum = rows_sum + rows_part(e, 0)
    qt_pass(1)
    rows_sum = rows_sum + rows_part(2, 1)
    for e in (1, 3):
        arrived(qt.at[e, 1], qt_r + groups * e + 1)
        rows_sum = rows_sum + rows_part(e, 1)
    rows_out[...] = rows_sum.astype(BF16)
    stores.append(fetch(rows_out, rows_raw))
    for e in range(1, ts):
        arrived(kv_tp.at[:, pl.ds(0, part)], kvt_r + e)
    for g in range(groups):
        for xr, e in order[:-1]:
            arrived(res_out.at[g, 0], res_r + g * X * ts + xr * ts + e)
    for copy in stores:
        copy.wait()
    for copy, when in pending:
        if when is None:
            copy.wait_send()
        else:
            pl.when(when)(copy.wait_send)


def widen_kernel(
    pieces, rows_raw, weight_raw, kv_raw, grad_rows, grad_weight, grad_keys, grad_values,
    rows_in, weight_in, kv_in, weight_out, kv_out, in_sem, out_sem,
):
    step = weight_raw.shape[0] // pieces
    outs = []

    def start(source, dest, sem):
        copy = pltpu.make_async_copy(source, dest, sem)
        copy.start()
        return copy

    spans = [pl.ds(i * step, step) for i in range(pieces)]
    weight_loads = [
        start(weight_raw.at[span], weight_in.at[span], in_sem.at[3 + i])
        for i, span in enumerate(spans)
    ]
    kv_loads = [start(kv_raw.at[i], kv_in.at[i], in_sem.at[i]) for i in range(2)]
    rows_load = start(rows_raw, rows_in, in_sem.at[2])
    for i, span in enumerate(spans):
        weight_loads[i].wait()
        weight_out[span] = weight_in[span].astype(F32)
        outs.append(start(weight_out.at[span], grad_weight.at[span], out_sem.at[3 + i]))
    for i, out in enumerate((grad_keys, grad_values)):
        kv_loads[i].wait()
        kv_out[i] = kv_in[i].astype(F32)
        outs.append(start(kv_out.at[i], out, out_sem.at[i]))
    rows_load.wait()
    outs.append(start(rows_in, grad_rows, out_sem.at[2]))
    for copy in outs:
        copy.wait()


def fused(target, gain, w_query, queries, keys, values, attn_out, grad_out):
    ts = lax.axis_size("tp")
    rows, width = queries.shape
    src = keys.shape[0]
    heads = width // HEAD_DIM
    hd = HEAD_DIM
    groups, gcols = heads // X, X * rows
    feats = target.shape[1]
    feat = feats // (ZS * X)
    part = src // ts
    vmem, hbm = pl.BlockSpec(memory_space=pltpu.VMEM), pl.BlockSpec(memory_space=pl.ANY)
    part_shape = pltpu.VMEM((groups, ZS, hd, gcols), BF16)
    raw = pl.pallas_call(
        functools.partial(fused_kernel, ts, heads),
        out_shape=(
            jax.ShapeDtypeStruct((rows, feats), BF16),
            jax.ShapeDtypeStruct((feat, width * ts), BF16),
            jax.ShapeDtypeStruct((2, part, keys.shape[1]), BF16),
        ),
        in_specs=[vmem, vmem, hbm, hbm, hbm, hbm, hbm, hbm],
        out_specs=(hbm,) * 3,
        scratch_shapes=[
            pltpu.VMEM((groups, ZS, gcols, hd), BF16),
            pltpu.VMEM((groups, ZS, gcols, hd), BF16),
            pltpu.VMEM((groups, gcols, hd), BF16),
            pltpu.VMEM((X * src, hd), BF16),
            pltpu.VMEM((X * src, hd), BF16),
            pltpu.VMEM((hd, X * src), BF16),
            pltpu.VMEM((ZS, groups, 1, gcols), F32),
            pltpu.VMEM((X * src, gcols), F32),
            pltpu.VMEM((X * src, groups * ZS * gcols), BF16),
            pltpu.VMEM((X * src, groups * ZS * gcols), BF16),
            part_shape, part_shape, part_shape, part_shape,
            pltpu.VMEM((ZS, ZS, groups, 2, gcols), F32),
            pltpu.VMEM((2, X * src, hd), F32),
            pltpu.VMEM((2, src, hd), BF16),
            pltpu.VMEM((2, src, hd), BF16),
            pltpu.VMEM((2, src, hd), BF16),
            pltpu.VMEM((ts, rows, 128), F32),
            pltpu.VMEM((feats, rows), BF16),
            pltpu.VMEM((X * ts, feat, ZS * X * rows), BF16),
            pltpu.VMEM((groups, ZS, rows, X * hd), BF16),
            pltpu.VMEM((ts, groups, rows, X * hd), BF16),
            pltpu.VMEM((groups, ZS * X * rows, hd), BF16),
            pltpu.VMEM((ts, feats, width), BF16),
            pltpu.VMEM((groups, X * ts, feat, hd), BF16),
            pltpu.VMEM((rows, feats), BF16),
            pltpu.SemaphoreType.DMA((240,)),
            pltpu.SemaphoreType.DMA((190,)),
            pltpu.SemaphoreType.DMA((8 + 3 * heads + ts,)),
        ],
        compiler_params=pltpu.CompilerParams(
            collective_id=0, has_side_effects=True, vmem_limit_bytes=60 * 2**20
        ),
    )(target, gain.reshape(1, feats), w_query, queries, keys, values, attn_out, grad_out)
    return pl.pallas_call(
        functools.partial(widen_kernel, PIECES),
        out_shape=(
            jax.ShapeDtypeStruct((rows, feats), BF16),
            jax.ShapeDtypeStruct((feat, width * ts), F32),
            jax.ShapeDtypeStruct((part, keys.shape[1]), F32),
            jax.ShapeDtypeStruct((part, keys.shape[1]), F32),
        ),
        in_specs=[hbm] * 3,
        out_specs=(hbm,) * 4,
        scratch_shapes=[
            pltpu.VMEM((rows, feats), BF16),
            pltpu.VMEM((feat, width * ts), BF16),
            pltpu.VMEM((2, part, keys.shape[1]), BF16),
            pltpu.VMEM((feat, width * ts), F32),
            pltpu.VMEM((2, part, keys.shape[1]), F32),
            pltpu.SemaphoreType.DMA((3 + PIECES,)),
            pltpu.SemaphoreType.DMA((3 + PIECES,)),
        ],
    )(*raw)


def fits(mesh):
    sp, tp = mesh.shape["sp"], mesh.shape["tp"]
    feat = WIDTH // (sp * tp)
    heads = HEADS // tp
    return tp == KV_HEADS and sp == ZS * X and feat % 128 == 0 and heads == 2 * X


def solution(mesh):
    return jax.shard_map(
        fused if fits(mesh) else local,
        mesh=mesh,
        in_specs=(
            P("sp", "tp"),
            P("tp"),
            P("tp", None),
            P("sp", "tp"),
            P("sp", None),
            P("sp", None),
            P("sp", "tp"),
            P("sp", "tp"),
        ),
        out_specs=(
            P("sp", "tp"),
            P(("tp", "sp"), None),
            P(("sp", "tp"), None),
            P(("sp", "tp"), None),
        ),
        check_vma=False,
    )
```

```python
import functools
import math

import jax
import jax.numpy as jnp
from jax import lax
from jax.experimental import pallas as pl
from jax.experimental.pallas import tpu as pltpu
from jax.sharding import PartitionSpec as P

WIDTH = 4096
HEADS = 16
KV_HEADS = 4
HEAD_DIM = 256


norm_eps = 1e-06


def merged(part, axis, combine):
    gathered = jax.tree.map(lambda a: lax.all_gather(a, axis), part)

    def take(source):
        return jax.tree.map(lambda a: lax.dynamic_index_in_dim(a, source, 0, False), gathered)

    return lax.fori_loop(
        1, lax.axis_size(axis), lambda source, state: combine(state, take(source)), take(0)
    )


def join_stats(first_part, second_part):
    row_peak = jnp.maximum(first_part[0], second_part[0])
    summed = first_part[1] * jnp.exp(first_part[0] - row_peak) + second_part[1] * jnp.exp(
        second_part[0] - row_peak
    )
    return (row_peak, summed, first_part[2] + second_part[2])


def local(target, gain, w_query, queries, keys, values, attn_out, grad_out):
    local_heads = queries.shape[1] // HEAD_DIM
    group_size = HEADS // KV_HEADS
    score_scale = HEAD_DIM ** (-0.5)
    own_rows = queries.shape[0]
    src_rows = keys.shape[0]
    kv_index = lax.axis_index("tp") * local_heads // group_size
    key_own = lax.dynamic_slice_in_dim(keys, kv_index * HEAD_DIM, HEAD_DIM, 1)
    value_own = lax.dynamic_slice_in_dim(values, kv_index * HEAD_DIM, HEAD_DIM, 1)
    out_heads = attn_out.reshape(own_rows, local_heads, HEAD_DIM).astype(jnp.float32)
    grad_heads = grad_out.reshape(own_rows, local_heads, HEAD_DIM).astype(jnp.float32)
    delta_own = jnp.sum(out_heads * grad_heads, axis=2)
    empty_sum = jnp.zeros((src_rows, HEAD_DIM), jnp.float32)
    total_rows = own_rows * lax.axis_size("sp")
    position = lax.axis_index("sp") * own_rows
    delta_full = lax.dynamic_update_slice_in_dim(
        jnp.zeros((total_rows, local_heads), jnp.float32), delta_own, position, 0
    )
    query_all, grad_all = (
        lax.all_gather(queries, "sp", axis=0, tiled=True),
        lax.all_gather(grad_out, "sp", axis=0, tiled=True),
    )
    block_rows = math.gcd(total_rows, 512)
    block_count = total_rows // block_rows
    query_blocks = query_all.reshape(block_count, block_rows, local_heads, HEAD_DIM)
    grad_blocks = grad_all.reshape(block_count, block_rows, local_heads, HEAD_DIM)

    def block_stats(query_block):
        scores = (
            jnp.einsum("qhd,sd->hqs", query_block, key_own, preferred_element_type=jnp.float32)
            * score_scale
        )
        row_peak = jnp.max(scores, axis=2)
        row_total = jnp.sum(jnp.exp(scores - row_peak[:, :, None]), axis=2)
        return (row_peak, row_total)

    peaks, totals = lax.map(block_stats, query_blocks)
    peaks, totals, delta_full = merged((peaks, totals, delta_full), "sp", join_stats)
    log_totals = peaks + jnp.log(totals)
    delta_blocks = delta_full.reshape(block_count, block_rows, local_heads)

    def block_grads(running, inputs):
        query_block, grad_block, delta_block, log_block = inputs
        scores = (
            jnp.einsum("qhd,sd->hqs", query_block, key_own, preferred_element_type=jnp.float32)
            * score_scale
        )
        weights = jnp.exp(scores - log_block[:, :, None])
        grad_weights = jnp.einsum(
            "qhd,sd->hqs", grad_block, value_own, preferred_element_type=jnp.float32
        )
        delta_cols = jnp.transpose(delta_block)
        grad_scores = (weights * (grad_weights - delta_cols[:, :, None]) * score_scale).astype(
            jnp.bfloat16
        )
        key_sum = running[0] + jnp.einsum(
            "hqs,qhd->sd", grad_scores, query_block, preferred_element_type=jnp.float32
        )
        value_sum = running[1] + jnp.einsum(
            "hqs,qhd->sd",
            weights.astype(jnp.bfloat16),
            grad_block,
            preferred_element_type=jnp.float32,
        )
        query_part = jnp.einsum(
            "hqs,sd->qhd", grad_scores, key_own, preferred_element_type=jnp.float32
        )
        return ((key_sum, value_sum), query_part)

    (key_sum, value_sum), query_parts = lax.scan(
        block_grads, (empty_sum, empty_sum), (query_blocks, grad_blocks, delta_blocks, log_totals)
    )
    query_parts = query_parts.reshape(total_rows, 1, local_heads * HEAD_DIM)
    received = lax.all_to_all(
        query_parts.astype(jnp.bfloat16), "sp", split_axis=0, concat_axis=1, tiled=True
    ).astype(query_parts.dtype)
    query_grad = jnp.sum(received, axis=1)
    key_cols = key_sum.reshape(src_rows, 1, HEAD_DIM)
    value_cols = value_sum.reshape(src_rows, 1, HEAD_DIM)
    key_parts, value_parts = (
        lax.all_to_all(
            key_cols.astype(jnp.bfloat16), "tp", split_axis=0, concat_axis=1, tiled=True
        ).astype(key_cols.dtype),
        lax.all_to_all(
            value_cols.astype(jnp.bfloat16), "tp", split_axis=0, concat_axis=1, tiled=True
        ).astype(value_cols.dtype),
    )
    part_rows = key_parts.shape[0]
    per_kv = key_parts.shape[1] // KV_HEADS
    grad_keys = (
        key_parts.reshape(part_rows, KV_HEADS, per_kv, HEAD_DIM)
        .sum(axis=2)
        .reshape(part_rows, KV_HEADS * HEAD_DIM)
    )
    grad_values = (
        value_parts.reshape(part_rows, KV_HEADS, per_kv, HEAD_DIM)
        .sum(axis=2)
        .reshape(part_rows, KV_HEADS * HEAD_DIM)
    )
    query_grad = query_grad.astype(jnp.bfloat16)
    query_all_heads = lax.all_gather(query_grad, "tp", axis=1, tiled=True)
    grad_rows = lax.dot_general(
        query_all_heads, w_query, (((1,), (1,)), ((), ())), preferred_element_type=jnp.float32
    ).astype(jnp.bfloat16)
    target_wide = target.astype(jnp.float32)
    squares = lax.psum(jnp.sum(target_wide * target_wide, axis=1), "tp")
    inverse = lax.rsqrt(squares / WIDTH + norm_eps)
    normed = (target_wide * inverse[:, None] * gain).astype(jnp.bfloat16)
    grad_weight = lax.psum_scatter(
        lax.dot_general(
            normed, query_all_heads, (((0,), (0,)), ((), ())), preferred_element_type=jnp.float32
        ).astype(jnp.bfloat16),
        "sp",
        scatter_dimension=0,
        tiled=True,
    ).astype(jnp.float32)
    return (grad_rows, grad_weight, grad_keys, grad_values)


MESH = pl.DeviceIdType.MESH
BF16, F32 = jnp.bfloat16, jnp.float32
NT = (((1,), (1,)), ((), ()))
X = 2
ZS = 4
CHUNK = 512
PIECES = 4


def fused_kernel(
    ts, heads,
    target, gain, w_query, queries, keys, values, attn_out, grad_out,
    rows_raw, weight_raw, kv_raw,
    qs, dos, outs, kbuf, vbuf, ktr, delta, sbuf, pbuf, dsbuf, qpart, part_in,
    side_out, side_in, stat, ksum, kv_out, kv_in, kv_tp, sq, ntr, nall,
    dqrow, qt, dqg, wbuf, res_out, rows_out, send, recv, local_sem,
):
    rows = queries.shape[0]
    src = keys.shape[0]
    hd = HEAD_DIM
    width = heads * hd
    groups = heads // X
    half = width // X
    gcols = X * rows
    part = src // ts
    feat = target.shape[1] // (ZS * X)
    scale = hd ** (-0.5)
    sp, tp = lax.axis_index("sp"), lax.axis_index("tp")
    z, x = sp // X, sp % X
    core = tp % 2
    side = z // 2
    outer = 1 - (z + side) % 2
    inner = outer == 0
    edge = outer > 0
    z_mate, z_oin, z_oout = 1 + 4 * side - z, 2 - side, 3 - 3 * side
    sib = tp + 1 - 2 * core
    tps = [tp, sib, (tp + 2) % ts, (sib + 2) % ts]
    x_off = 1 - x
    slots_z = [z, z_mate, z_oin, z_oout]
    swap = (1, 0, 2, 3)
    far = 2 + outer

    def dev(zz, xx, tt):
        return (zz * X + xx, tt)

    mate, oin, oout = (dev(a, x, tp) for a in (z_mate, z_oin, z_oout))
    xpeer, y_peer, sib_peer = dev(z, x_off, tp), dev(z, x, tps[2]), dev(z, x, sib)
    counts = {"send": 0, "recv": 0, "local": 0}

    def take(kind, n=1):
        at = counts[kind]
        counts[kind] += n
        return at

    def copy_of(source, dest, device, si, ri):
        return pltpu.make_async_remote_copy(
            src_ref=source, dst_ref=dest, send_sem=send.at[si], recv_sem=recv.at[ri],
            device_id=device, device_id_type=MESH,
        )

    bins = []
    small = {1: take("send"), groups: take("send")}

    def planned(source, dest, device, ri, when):
        size = math.prod(source.shape) * jnp.dtype(source.dtype).itemsize // (2 * width)
        if source.dtype == F32 and source.shape[0] != rows:
            return copy_of(source, dest, device, small[math.prod(source.shape[:-2])], ri)
        for entry in bins:
            if entry["when"] is when and entry["size"] + size <= wbuf.shape[1]:
                break
        else:
            entry = {"when": when, "size": 0, "sem": take("send")}
            bins.append(entry)
        entry["size"] += size
        return copy_of(source, dest, device, entry["sem"], ri)

    def push(source, dest, device, ri, when=None):
        copy = planned(source, dest, device, ri, when)
        if when is None:
            copy.start()
        else:
            pl.when(when)(copy.start)

    def arrived(view, ri):
        copy_of(view, view, xpeer, 0, ri).wait_recv()

    def fetch(source, dest, sem=None):
        sem = take("local") if sem is None else sem
        copy = pltpu.make_async_copy(source, dest, local_sem.at[sem])
        copy.start()
        return copy

    def loaded(view, sem):
        pltpu.make_async_copy(view, view, local_sem.at[sem]).wait()

    def head_of(g, xx):
        return xx * groups + g

    head_col = pl.ds(pl.multiple_of(tp * hd, hd), hd)
    q_l, d_l, o_l, w_l = (take("local") for _ in range(4))
    for sem, ref, buf in ((q_l, queries, qs), (d_l, grad_out, dos), (o_l, attn_out, outs)):
        for g in range(groups):
            for xx in range(X):
                view = buf.at[g] if buf is outs else buf.at[g, 0]
                view = view.at[pl.ds(xx * rows, rows)]
                fetch(ref.at[:, pl.ds(head_of(g, xx) * hd, hd)], view, sem)
    k_load = fetch(keys.at[:, head_col], kbuf.at[pl.ds(0, src)])
    v_load = fetch(values.at[:, head_col], vbuf.at[pl.ds(0, src)])
    for e, t in enumerate(tps):
        w_cols = pl.ds(pl.multiple_of(t * width, width), width)
        fetch(w_query.at[:, w_cols], wbuf.at[e], w_l)

    barrier = pltpu.get_barrier_semaphore()
    peers = [dev(a, x, tp) for a in slots_z[1:]] + [dev(a, x_off, tp) for a in slots_z]
    peers += [dev(z, xx, t) for xx in (x, x_off) for t in tps[1:]]
    for peer in peers:
        pl.semaphore_signal(barrier, inc=1, device_id=peer, device_id_type=MESH)

    wide = target[...].astype(F32)
    sq[0] = jnp.broadcast_to(jnp.sum(wide * wide, axis=1, keepdims=True), (rows, 128))
    loaded(dos.at[pl.ds(0, groups), 0], d_l)
    loaded(outs, o_l)
    for g in range(groups):
        dot = jnp.sum(dos[g, 0].astype(F32) * outs[g].astype(F32), axis=1, keepdims=True)
        delta[0, g] = jnp.broadcast_to(dot, (gcols, 128)).T[:1]
    loaded(qs.at[pl.ds(0, groups), 0], q_l)
    k_load.wait()
    v_load.wait()
    pl.semaphore_wait(barrier, len(peers))

    q_r, d_r = take("recv", ZS * groups), take("recv", ZS * groups)
    delta_r, sq_r = take("recv"), take("recv")
    k_r, v_r = take("recv"), take("recv")

    def gather(buf, base, g, a, b, device, when=None):
        push(buf.at[g, a], buf.at[g, b], device, base + ZS * g + b, when)

    push(delta.at[0], delta.at[1], mate, delta_r)
    push(delta.at[0], delta.at[far], oin, delta_r)
    push(delta.at[0], delta.at[far], oout, delta_r)
    for e in range(1, ts):
        push(sq.at[0], sq.at[e], dev(z, x, tps[e]), sq_r)
    gather(qs, q_r, 0, 0, 1, mate)
    gather(qs, q_r, 0, 0, 2, oin, inner)
    push(kbuf.at[pl.ds(0, src)], kbuf.at[pl.ds(src, src)], xpeer, k_r)
    gather(dos, d_r, 0, 0, 1, mate)
    gather(dos, d_r, 0, 0, 2, oin, inner)
    push(vbuf.at[pl.ds(0, src)], vbuf.at[pl.ds(src, src)], xpeer, v_r)
    for g in range(1, groups):
        gather(qs, q_r, g, 0, 1, mate)
        gather(dos, d_r, g, 0, 1, mate)

    ktr[:, :src] = kbuf[:src].T
    arrived(sq.at[pl.ds(1, ts - 1)], sq_r)
    total = sq[0]
    for e in range(1, ts):
        total = total + sq[e]
    inverse = lax.rsqrt(total[:, :1] / (target.shape[1] * ts) + norm_eps)
    normed = target[...].astype(F32) * inverse * gain[...]
    ntr[...] = normed.T.astype(BF16)

    def feature_rows(zz, xx):
        return pl.ds(pl.multiple_of((zz * X + xx) * feat, feat), feat)

    def lanes(slot, xx):
        return pl.ds(pl.multiple_of((slot * X + xx) * rows, rows), rows)

    n_r, n_sib = take("recv"), take("recv")
    n_in = {ts: take("recv"), 2: take("recv"), ts + 2: take("recv")}

    def n_send(zz, slot, xr):
        xx = (x, x_off)[xr]
        push(
            ntr.at[feature_rows(zz, xx)], nall.at[0, :, lanes(slot, x)], dev(zz, xx, tp),
            n_r,
        )

    def n_pass(i, to, device, when=None):
        push(nall.at[i], nall.at[to], device, n_in.get(to, n_sib), when)

    def n_relay(when):
        @pl.when(when)
        def _():
            arrived(nall.at[0], n_in[ts])

        n_pass(ts, ts + 2, y_peer, when)
        n_pass(ts, ts + 1, sib_peer, when)

    nall[0, :, lanes(0, x)] = ntr[feature_rows(z, x)]

    def relay(g, a, b, device):
        for buf, base in ((qs, q_r), (dos, d_r)):
            copy = planned(buf.at[g, a], buf.at[g, b], device, base + ZS * g + b, inner)

            @pl.when(inner)
            def _():
                arrived(buf.at[g, a], base + ZS * g + a)
                copy.start()

    def gathered(g, a):
        @pl.when(edge)
        def _():
            arrived(qs.at[g, a], q_r + ZS * g + a)
            arrived(dos.at[g, a], d_r + ZS * g + a)

    chunks = X * src // CHUNK

    def scores_of(g, j):
        def step(c, peak):
            span = pl.ds(pl.multiple_of(c * CHUNK, CHUNK), CHUNK)
            s = lax.dot_general(kbuf[span], qs[g, j], NT, preferred_element_type=F32)
            sbuf[span] = s
            return jnp.maximum(peak, jnp.max(s, axis=0, keepdims=True))

        return lax.fori_loop(0, chunks, step, jnp.full((1, gcols), -jnp.inf, F32), unroll=True)

    def grads_of(g, j, peak):
        own_delta = delta[j, g]
        lane_span = pl.ds((g * ZS + j) * gcols, gcols)

        def step(c, total):
            span = pl.ds(pl.multiple_of(c * CHUNK, CHUNK), CHUNK)
            p = jnp.exp((sbuf[span] - peak) * scale)
            dp = lax.dot_general(vbuf[span], dos[g, j], NT, preferred_element_type=F32)
            pbuf[span, lane_span] = p.astype(BF16)
            dsbuf[span, lane_span] = (p * (dp - own_delta) * scale).astype(BF16)
            return total + jnp.sum(p, axis=0, keepdims=True)

        total = lax.fori_loop(0, chunks, step, jnp.zeros((1, gcols), F32), unroll=True)
        stat[0, slots_z[j], g, 0:1] = peak * scale
        stat[0, slots_z[j], g, 1:2] = total
        qpart[g, j] = jnp.dot(ktr[...], dsbuf[:, lane_span], preferred_element_type=F32).astype(BF16)

    stat_r = take("recv", groups * (ZS + 1))
    part_r, side_r = take("recv", groups * ZS), take("recv", groups * ZS)

    def mate_stat(g, j):
        return stat_r + (ZS + 1) * g + j

    def share(g, j):
        zt = slots_z[j]
        for device in (oin, oout):
            push(stat.at[0, zt, g], stat.at[far, zt, g], device, mate_stat(g, ZS))
        push(stat.at[0, zt, g], stat.at[1, zt, g], mate, mate_stat(g, j))
        to = swap[j]
        push(qpart.at[g, j], part_in.at[g, to], mate, part_r + ZS * g + to, edge)

    def process(g, j):
        grads_of(g, j, scores_of(g, j))
        share(g, j)

    def weights_of(g, j, sources):
        zt = slots_z[j]
        tops = [stat[e, zt, g, 0:1] for e in sources]
        top = functools.reduce(jnp.maximum, tops)
        scaled = [jnp.exp(m - top) for m in tops]
        summed = sum(f * stat[e, zt, g, 1:2] for e, f in zip(sources, scaled))
        return top, scaled, summed

    def stats_came(g):
        arrived(stat.at[pl.ds(2, 2), pl.ds(0, ZS), g], mate_stat(g, ZS))

    def side_sum(g, j):
        @pl.when(inner)
        def _():
            arrived(stat.at[0, 0, 0], mate_stat(g, swap[j]))
            arrived(part_in.at[g, j], part_r + ZS * g + j)
            _, (f_own, f_mate), _ = weights_of(g, j, (0, 1))
            near_part = qpart[g, j].astype(F32) * f_own + part_in[g, j].astype(F32) * f_mate
            side_out[g, j] = near_part.astype(BF16)

        to = (j + 2) % ZS
        push(side_out.at[g, j], side_in.at[g, to], oin, side_r + ZS * g + to, inner)

    row_r, g_r, xs_r = take("recv", groups), take("recv", groups), take("recv", groups * ZS)
    qt_r, qs_r = take("recv", groups), take("recv", groups)

    def rows_of(slot, xx):
        return pl.ds(pl.multiple_of((slot * X + xx) * rows, rows), rows)

    def lanes_of(xx):
        return pl.ds(pl.multiple_of(xx * hd, hd), hd)

    def spread(g, j, when):
        push(
            dqrow.at[g, j, :, lanes_of(x_off)], dqg.at[g, rows_of(j, x)], xpeer,
            xs_r + ZS * g + j, when,
        )

        @pl.when(when)
        def _():
            dqg[g, rows_of(j, x)] = dqrow[g, j, :, lanes_of(x)]

    def qt_sends(g, when):
        push(dqrow.at[g, 0], qt.at[2, g], y_peer, qt_r + g, when)
        push(dqrow.at[g, 0], qt.at[1, g], sib_peer, qs_r + g, when)

    def reduce_rows(g, j):
        @pl.when(inner)
        def _():
            arrived(side_in.at[g, j], side_r + ZS * g + j)
            top, _, summed = weights_of(g, j, range(ZS))
            near_top, far_top = (weights_of(g, j, pair)[0] for pair in ((0, 1), (2, 3)))
            grad_t = side_out[g, j].astype(F32) * (jnp.exp(near_top - top) / summed)
            grad_t = grad_t + side_in[g, j].astype(F32) * (jnp.exp(far_top - top) / summed)
            grad_own = grad_t.T.astype(BF16)
            for xx in range(X):
                dqrow[g, j, :, pl.ds(xx * hd, hd)] = grad_own[xx * rows : (xx + 1) * rows]

        spread(g, j, inner)
        if j == 0:
            qt_sends(g, inner)

    def joined(g, j):
        arrived(dqg.at[g, pl.ds(0, rows)], xs_r + ZS * g + j)

    def block_of(g, j):
        return dqg.at[g, pl.ds(j * X * rows, X * rows)]

    def hand(g, j):
        @pl.when(inner)
        def _():
            joined(g, j)

        push(block_of(g, j), block_of(g, swap[j]), mate, g_r + g, inner)

    def hand_rows(g):
        push(
            dqrow.at[g, 1, :, lanes_of(x_off)], dqrow.at[g, 0, :, lanes_of(x_off)], mate,
            row_r + g, inner,
        )

    def hand_direct(g):
        for xx in (x_off, x):
            push(
                dqrow.at[g, 1, :, lanes_of(xx)], dqg.at[g, rows_of(0, x)], dev(z_mate, xx, tp),
                g_r + g, inner,
            )

    def dkv():
        pairs = [(g, j) for g in range(groups) for j in range(ZS)]

        def stacked(e, i):
            rows_in = [stat[e, slots_z[j], g, i : i + 1] for g, j in pairs]
            return jnp.concatenate(rows_in, axis=0)

        tops = [stacked(e, 0) for e in range(ZS)]
        top = functools.reduce(jnp.maximum, tops)
        scaled = [jnp.exp(m - top) for m in tops]
        summed = sum(f * stacked(e, 1) for e, f in enumerate(scaled))
        ratios = (scaled[0] / summed).T
        for n in range(0, len(pairs), 2):
            held = []
            for i, buf in enumerate((qs, dos)):
                pieces = [
                    (buf[g, j].astype(F32) * ratios[:, n + k : n + k + 1]).astype(BF16)
                    for k, (g, j) in enumerate(pairs[n : n + 2])
                ]
                held.append(jnp.concatenate(pieces, axis=0))
            span = pl.ds(n * gcols, 2 * gcols)
            for i, left in enumerate((dsbuf, pbuf)):
                piece = jnp.dot(left[:, span], held[i], preferred_element_type=F32)
                ksum[i] = piece if n == 0 else ksum[i] + piece

    kvx_r, kvt_r = take("recv"), take("recv")
    quarter = src // 4
    stores = []

    def kvx(first, last, when):
        for n in range(first, last):
            piece = pl.ds(n % 4 * quarter, quarter)
            push(kv_out.at[n // 4, piece], kv_in.at[n // 4, piece], xpeer, kvx_r, when)

    def part_rows(t):
        return pl.ds(pl.multiple_of(t * part, part), part)

    def kv_finish(when):
        @pl.when(when)
        def _():
            arrived(kv_in, kvx_r)
            for i in range(2):
                kv_tp[i] = (ksum[i, :src] + kv_in[i].astype(F32)).astype(BF16)

        for e in range(1, ts):
            push(
                kv_tp.at[:, part_rows(tps[e])], kv_raw.at[:, :, head_col], dev(z, x, tps[e]),
                kvt_r, when,
            )

    res_r = take("recv")

    def res_push(g, xr, e, when=None):
        k = xr * ts + e
        at = pl.ds(pl.multiple_of(tp * width + x * half + g * hd, hd), hd)
        if k:
            push(
                res_out.at[g, k], weight_raw.at[:, at], dev(z, (x, x_off)[xr], tps[e]),
                res_r, when,
            )
        else:
            stores.append(fetch(res_out.at[g, 0], weight_raw.at[:, at]))

    def project(g):
        for xr in (1, 0):
            block = nall[pl.ds(xr * ts, ts)].reshape(ts * feat, ZS * X * rows)
            result = jnp.dot(block, dqg[g], preferred_element_type=F32).astype(BF16)
            for e in range(ts):
                res_out[g, xr * ts + e] = result[e * feat : (e + 1) * feat]

    def ready(g):
        @pl.when(edge)
        def _():
            arrived(dqg.at[g], g_r + g)

    def own_rows(g):
        @pl.when(edge)
        def _():
            dqrow[g, 0, :, lanes_of(x)] = dqg[g, rows_of(0, x)]
            arrived(dqrow.at[g, 0, :, pl.ds(0, hd)], row_r + g)

        qt_sends(g, edge)

    def qt_pass(g):
        arrived(qt.at[2, g], qt_r + g)
        push(qt.at[2, g], qt.at[3, g], sib_peer, qs_r + g)

    def rows_part(e, g):
        left = dqrow[g, 0] if e == 0 else qt[e, g]
        total = 0.0
        for xx in range(X):
            w_cols = wbuf[e, :, pl.ds(head_of(g, xx) * hd, hd)]
            total = total + lax.dot_general(
                left[:, xx * hd : (xx + 1) * hd], w_cols, NT, preferred_element_type=F32
            )
        return total

    relay(0, 1, 3, oin)
    relay(0, 2, 2, mate)
    for g in range(1, groups):
        gather(qs, q_r, g, 0, 2, oin, inner)
        gather(dos, d_r, g, 0, 2, oin, inner)
    arrived(kbuf.at[pl.ds(src, src)], k_r)
    ktr[:, src:] = kbuf[src:].T
    peak = scores_of(0, 0)
    arrived(vbuf.at[pl.ds(src, src)], v_r)
    relay(1, 1, 3, oin)
    grads_of(0, 0, peak)
    share(0, 0)
    relay(0, 3, 3, mate)
    arrived(delta.at[pl.ds(1, ZS - 1)], delta_r)
    gathered(0, 1)
    process(0, 1)
    for xr in range(X):
        n_send(z_oin, far, xr)
        n_send(z_oout, far, xr)
        n_send(z_mate, 1, xr)
    n_send(z, 0, 1)
    relay(1, 2, 2, mate)
    gathered(0, 2)
    process(0, 2)
    gathered(0, 3)
    process(0, 3)
    side_sum(0, 0)
    side_sum(0, 1)
    relay(1, 3, 3, mate)
    gathered(1, 1)
    side_sum(0, 2)
    arrived(nall.at[0, :, pl.ds(0, (ZS * X - 1) * rows)], n_r)
    n_pass(0, ts, xpeer)
    n_pass(0, 2, y_peer)
    n_pass(0, 1, sib_peer)
    process(1, 0)
    process(1, 1)
    side_sum(0, 3)
    gathered(1, 2)
    process(1, 2)
    n_relay(edge)
    gathered(1, 3)
    process(1, 3)
    @pl.when(inner)
    def _():
        stats_came(0)

    reduce_rows(0, 2)
    reduce_rows(0, 3)
    hand(0, 2)
    n_relay(inner)
    reduce_rows(0, 0)
    hand(0, 3)
    side_sum(1, 0)
    side_sum(1, 1)
    reduce_rows(0, 1)
    hand(0, 0)
    side_sum(1, 2)
    hand(0, 1)
    hand_rows(0)
    side_sum(1, 3)
    arrived(nall.at[0], n_in[2])
    n_pass(2, 3, sib_peer)
    arrived(nall.at[0], n_in[ts + 2])
    n_pass(ts + 2, ts + 3, sib_peer)
    @pl.when(edge)
    def _():
        for g in range(groups):
            for j in range(ZS):
                arrived(stat.at[0, 0, 0], mate_stat(g, j))
            stats_came(g)

    @pl.when(inner)
    def _():
        stats_came(1)

    reduce_rows(1, 2)
    reduce_rows(1, 3)
    @pl.when(inner)
    def _():
        arrived(nall.at[pl.ds(0, ts)], n_sib)

        project(0)

    for e in (3, 2):
        res_push(0, 1, e, inner)
    dkv()
    kv_out[...] = ksum[:, src:].astype(BF16)
    kvx(0, 8, edge)
    hand(1, 2)
    reduce_rows(1, 0)
    hand(1, 3)
    kvx(0, 1, inner)
    for e in (3, 2, 1):
        res_push(0, 0, e, inner)
    @pl.when(edge)
    def _():
        arrived(nall.at[pl.ds(0, ts)], n_sib)

    ready(0)
    @pl.when(edge)
    def _():
        project(0)

    for xr in (1, 0):
        for e in (3, 2, 1, 0):
            if xr or e:
                res_push(0, xr, e, edge)
    res_push(0, 0, 0)
    own_rows(0)
    hand(1, 0)
    reduce_rows(1, 1)
    hand_direct(1)
    hand_rows(1)
    kvx(1, 8, inner)

    @pl.when(inner)
    def _():
        joined(1, 1)

    for e in (1, 0):
        res_push(0, 1, e, inner)
    qt_pass(0)
    kv_finish(edge)
    ready(1)
    own_rows(1)
    project(1)
    for xr in (1, 0):
        for e in (3, 2, 1, 0):
            res_push(1, xr, e)
    kv_finish(inner)
    stores.append(fetch(kv_tp.at[:, part_rows(tp)], kv_raw.at[:, :, head_col]))
    loaded(wbuf, w_l)
    rows_sum = rows_part(0, 0) + rows_part(0, 1) + rows_part(2, 0)
    arrived(qt.at[pl.ds(0, 2), 0], qs_r)
    for e in (1, 3):
        rows_sum = rows_sum + rows_part(e, 0)
    qt_pass(1)
    rows_sum = rows_sum + rows_part(2, 1)
    arrived(qt.at[pl.ds(0, 2), 1], qs_r + 1)
    for e in (1, 3):
        rows_sum = rows_sum + rows_part(e, 1)
    rows_out[...] = rows_sum.astype(BF16)
    stores.append(fetch(rows_out, rows_raw))
    arrived(kv_raw.at[:, :, pl.ds(0, (ts - 1) * hd)], kvt_r)
    arrived(weight_raw.at[:, pl.ds(0, groups * (X * ts - 1) * hd)], res_r)
    for copy in stores:
        copy.wait()
    for sent, sem in ((stat.at[pl.ds(0, ZS - 1)], small[1]), (delta.at[pl.ds(1, ZS - 1)], small[groups])):
        copy_of(sent, sent, xpeer, sem, 0).wait_send()
    for entry in bins:
        sent = wbuf.at[0, pl.ds(0, entry["size"])]
        wait = copy_of(sent, sent, xpeer, entry["sem"], 0).wait_send
        wait() if entry["when"] is None else pl.when(entry["when"])(wait)
    assert counts["send"] <= send.shape[0] and counts["recv"] <= recv.shape[0]


def widen_kernel(
    pieces, rows_raw, weight_raw, kv_raw, grad_rows, grad_weight, grad_keys, grad_values,
    rows_in, weight_in, kv_in, weight_out, kv_out, in_sem, out_sem,
):
    step = weight_raw.shape[0] // pieces
    outs = []

    def start(source, dest, sem):
        copy = pltpu.make_async_copy(source, dest, sem)
        copy.start()
        return copy

    spans = [pl.ds(i * step, step) for i in range(pieces)]
    weight_loads = [
        start(weight_raw.at[span], weight_in.at[span], in_sem.at[3 + i])
        for i, span in enumerate(spans)
    ]
    kv_loads = [start(kv_raw.at[i], kv_in.at[i], in_sem.at[i]) for i in range(2)]
    rows_load = start(rows_raw, rows_in, in_sem.at[2])
    for i, span in enumerate(spans):
        weight_loads[i].wait()
        weight_out[span] = weight_in[span].astype(F32)
        outs.append(start(weight_out.at[span], grad_weight.at[span], out_sem.at[3 + i]))
    for i, out in enumerate((grad_keys, grad_values)):
        kv_loads[i].wait()
        kv_out[i] = kv_in[i].astype(F32)
        outs.append(start(kv_out.at[i], out, out_sem.at[i]))
    rows_load.wait()
    outs.append(start(rows_in, grad_rows, out_sem.at[2]))
    for copy in outs:
        copy.wait()


def fused(target, gain, w_query, queries, keys, values, attn_out, grad_out):
    ts = lax.axis_size("tp")
    rows, width = queries.shape
    src = keys.shape[0]
    heads = width // HEAD_DIM
    hd = HEAD_DIM
    groups, gcols = heads // X, X * rows
    feats = target.shape[1]
    feat = feats // (ZS * X)
    part = src // ts
    vmem, hbm = pl.BlockSpec(memory_space=pltpu.VMEM), pl.BlockSpec(memory_space=pl.ANY)
    part_shape = pltpu.VMEM((groups, ZS, hd, gcols), BF16)
    raw = pl.pallas_call(
        functools.partial(fused_kernel, ts, heads),
        out_shape=(
            jax.ShapeDtypeStruct((rows, feats), BF16),
            jax.ShapeDtypeStruct((feat, width * ts), BF16),
            jax.ShapeDtypeStruct((2, part, keys.shape[1]), BF16),
        ),
        in_specs=[vmem, vmem, hbm, hbm, hbm, hbm, hbm, hbm],
        out_specs=(hbm,) * 3,
        scratch_shapes=[
            pltpu.VMEM((groups, ZS, gcols, hd), BF16),
            pltpu.VMEM((groups, ZS, gcols, hd), BF16),
            pltpu.VMEM((groups, gcols, hd), BF16),
            pltpu.VMEM((X * src, hd), BF16),
            pltpu.VMEM((X * src, hd), BF16),
            pltpu.VMEM((hd, X * src), BF16),
            pltpu.VMEM((ZS, groups, 1, gcols), F32),
            pltpu.VMEM((X * src, gcols), F32),
            pltpu.VMEM((X * src, groups * ZS * gcols), BF16),
            pltpu.VMEM((X * src, groups * ZS * gcols), BF16),
            part_shape, part_shape, part_shape, part_shape,
            pltpu.VMEM((ZS, ZS, groups, 2, gcols), F32),
            pltpu.VMEM((2, X * src, hd), F32),
            pltpu.VMEM((2, src, hd), BF16),
            pltpu.VMEM((2, src, hd), BF16),
            pltpu.VMEM((2, src, hd), BF16),
            pltpu.VMEM((ts, rows, 128), F32),
            pltpu.VMEM((feats, rows), BF16),
            pltpu.VMEM((X * ts, feat, ZS * X * rows), BF16),
            pltpu.VMEM((groups, ZS, rows, X * hd), BF16),
            pltpu.VMEM((ts, groups, rows, X * hd), BF16),
            pltpu.VMEM((groups, ZS * X * rows, hd), BF16),
            pltpu.VMEM((ts, feats, width), BF16),
            pltpu.VMEM((groups, X * ts, feat, hd), BF16),
            pltpu.VMEM((rows, feats), BF16),
            pltpu.SemaphoreType.DMA((16,)),
            pltpu.SemaphoreType.DMA((76,)),
            pltpu.SemaphoreType.DMA((12,)),
        ],
        compiler_params=pltpu.CompilerParams(
            collective_id=0, has_side_effects=True, vmem_limit_bytes=60 * 2**20
        ),
    )(target, gain.reshape(1, feats), w_query, queries, keys, values, attn_out, grad_out)
    return pl.pallas_call(
        functools.partial(widen_kernel, PIECES),
        out_shape=(
            jax.ShapeDtypeStruct((rows, feats), BF16),
            jax.ShapeDtypeStruct((feat, width * ts), F32),
            jax.ShapeDtypeStruct((part, keys.shape[1]), F32),
            jax.ShapeDtypeStruct((part, keys.shape[1]), F32),
        ),
        in_specs=[hbm] * 3,
        out_specs=(hbm,) * 4,
        scratch_shapes=[
            pltpu.VMEM((rows, feats), BF16),
            pltpu.VMEM((feat, width * ts), BF16),
            pltpu.VMEM((2, part, keys.shape[1]), BF16),
            pltpu.VMEM((feat, width * ts), F32),
            pltpu.VMEM((2, part, keys.shape[1]), F32),
            pltpu.SemaphoreType.DMA((3 + PIECES,)),
            pltpu.SemaphoreType.DMA((3 + PIECES,)),
        ],
    )(*raw)


def fits(mesh):
    sp, tp = mesh.shape["sp"], mesh.shape["tp"]
    feat = WIDTH // (sp * tp)
    heads = HEADS // tp
    return tp == KV_HEADS and sp == ZS * X and feat % 128 == 0 and heads == 2 * X


def solution(mesh):
    return jax.shard_map(
        fused if fits(mesh) else local,
        mesh=mesh,
        in_specs=(
            P("sp", "tp"),
            P("tp"),
            P("tp", None),
            P("sp", "tp"),
            P("sp", None),
            P("sp", None),
            P("sp", "tp"),
            P("sp", "tp"),
        ),
        out_specs=(
            P("sp", "tp"),
            P(("tp", "sp"), None),
            P(("sp", "tp"), None),
            P(("sp", "tp"), None),
        ),
        check_vma=False,
    )
```

```python
import functools
import math

import jax
import jax.numpy as jnp
from jax import lax
from jax.experimental import pallas as pl
from jax.experimental.pallas import tpu as pltpu
from jax.sharding import PartitionSpec as P

WIDTH = 4096
HEADS = 16
KV_HEADS = 4
HEAD_DIM = 256


norm_eps = 1e-06


def merged(part, axis, combine):
    gathered = jax.tree.map(lambda a: lax.all_gather(a, axis), part)

    def take(source):
        return jax.tree.map(lambda a: lax.dynamic_index_in_dim(a, source, 0, False), gathered)

    return lax.fori_loop(
        1, lax.axis_size(axis), lambda source, state: combine(state, take(source)), take(0)
    )


def join_stats(first_part, second_part):
    row_peak = jnp.maximum(first_part[0], second_part[0])
    summed = first_part[1] * jnp.exp(first_part[0] - row_peak) + second_part[1] * jnp.exp(
        second_part[0] - row_peak
    )
    return (row_peak, summed, first_part[2] + second_part[2])


def local(target, gain, w_query, queries, keys, values, attn_out, grad_out):
    local_heads = queries.shape[1] // HEAD_DIM
    group_size = HEADS // KV_HEADS
    score_scale = HEAD_DIM ** (-0.5)
    own_rows = queries.shape[0]
    src_rows = keys.shape[0]
    kv_index = lax.axis_index("tp") * local_heads // group_size
    key_own = lax.dynamic_slice_in_dim(keys, kv_index * HEAD_DIM, HEAD_DIM, 1)
    value_own = lax.dynamic_slice_in_dim(values, kv_index * HEAD_DIM, HEAD_DIM, 1)
    out_heads = attn_out.reshape(own_rows, local_heads, HEAD_DIM).astype(jnp.float32)
    grad_heads = grad_out.reshape(own_rows, local_heads, HEAD_DIM).astype(jnp.float32)
    delta_own = jnp.sum(out_heads * grad_heads, axis=2)
    empty_sum = jnp.zeros((src_rows, HEAD_DIM), jnp.float32)
    total_rows = own_rows * lax.axis_size("sp")
    position = lax.axis_index("sp") * own_rows
    delta_full = lax.dynamic_update_slice_in_dim(
        jnp.zeros((total_rows, local_heads), jnp.float32), delta_own, position, 0
    )
    query_all, grad_all = (
        lax.all_gather(queries, "sp", axis=0, tiled=True),
        lax.all_gather(grad_out, "sp", axis=0, tiled=True),
    )
    block_rows = math.gcd(total_rows, 512)
    block_count = total_rows // block_rows
    query_blocks = query_all.reshape(block_count, block_rows, local_heads, HEAD_DIM)
    grad_blocks = grad_all.reshape(block_count, block_rows, local_heads, HEAD_DIM)

    def block_stats(query_block):
        scores = (
            jnp.einsum("qhd,sd->hqs", query_block, key_own, preferred_element_type=jnp.float32)
            * score_scale
        )
        row_peak = jnp.max(scores, axis=2)
        row_total = jnp.sum(jnp.exp(scores - row_peak[:, :, None]), axis=2)
        return (row_peak, row_total)

    peaks, totals = lax.map(block_stats, query_blocks)
    peaks, totals, delta_full = merged((peaks, totals, delta_full), "sp", join_stats)
    log_totals = peaks + jnp.log(totals)
    delta_blocks = delta_full.reshape(block_count, block_rows, local_heads)

    def block_grads(running, inputs):
        query_block, grad_block, delta_block, log_block = inputs
        scores = (
            jnp.einsum("qhd,sd->hqs", query_block, key_own, preferred_element_type=jnp.float32)
            * score_scale
        )
        weights = jnp.exp(scores - log_block[:, :, None])
        grad_weights = jnp.einsum(
            "qhd,sd->hqs", grad_block, value_own, preferred_element_type=jnp.float32
        )
        delta_cols = jnp.transpose(delta_block)
        grad_scores = (weights * (grad_weights - delta_cols[:, :, None]) * score_scale).astype(
            jnp.bfloat16
        )
        key_sum = running[0] + jnp.einsum(
            "hqs,qhd->sd", grad_scores, query_block, preferred_element_type=jnp.float32
        )
        value_sum = running[1] + jnp.einsum(
            "hqs,qhd->sd",
            weights.astype(jnp.bfloat16),
            grad_block,
            preferred_element_type=jnp.float32,
        )
        query_part = jnp.einsum(
            "hqs,sd->qhd", grad_scores, key_own, preferred_element_type=jnp.float32
        )
        return ((key_sum, value_sum), query_part)

    (key_sum, value_sum), query_parts = lax.scan(
        block_grads, (empty_sum, empty_sum), (query_blocks, grad_blocks, delta_blocks, log_totals)
    )
    query_parts = query_parts.reshape(total_rows, 1, local_heads * HEAD_DIM)
    received = lax.all_to_all(
        query_parts.astype(jnp.bfloat16), "sp", split_axis=0, concat_axis=1, tiled=True
    ).astype(query_parts.dtype)
    query_grad = jnp.sum(received, axis=1)
    key_cols = key_sum.reshape(src_rows, 1, HEAD_DIM)
    value_cols = value_sum.reshape(src_rows, 1, HEAD_DIM)
    key_parts, value_parts = (
        lax.all_to_all(
            key_cols.astype(jnp.bfloat16), "tp", split_axis=0, concat_axis=1, tiled=True
        ).astype(key_cols.dtype),
        lax.all_to_all(
            value_cols.astype(jnp.bfloat16), "tp", split_axis=0, concat_axis=1, tiled=True
        ).astype(value_cols.dtype),
    )
    part_rows = key_parts.shape[0]
    per_kv = key_parts.shape[1] // KV_HEADS
    grad_keys = (
        key_parts.reshape(part_rows, KV_HEADS, per_kv, HEAD_DIM)
        .sum(axis=2)
        .reshape(part_rows, KV_HEADS * HEAD_DIM)
    )
    grad_values = (
        value_parts.reshape(part_rows, KV_HEADS, per_kv, HEAD_DIM)
        .sum(axis=2)
        .reshape(part_rows, KV_HEADS * HEAD_DIM)
    )
    query_grad = query_grad.astype(jnp.bfloat16)
    query_all_heads = lax.all_gather(query_grad, "tp", axis=1, tiled=True)
    grad_rows = lax.dot_general(
        query_all_heads, w_query, (((1,), (1,)), ((), ())), preferred_element_type=jnp.float32
    ).astype(jnp.bfloat16)
    target_wide = target.astype(jnp.float32)
    squares = lax.psum(jnp.sum(target_wide * target_wide, axis=1), "tp")
    inverse = lax.rsqrt(squares / WIDTH + norm_eps)
    normed = (target_wide * inverse[:, None] * gain).astype(jnp.bfloat16)
    grad_weight = lax.psum_scatter(
        lax.dot_general(
            normed, query_all_heads, (((0,), (0,)), ((), ())), preferred_element_type=jnp.float32
        ).astype(jnp.bfloat16),
        "sp",
        scatter_dimension=0,
        tiled=True,
    ).astype(jnp.float32)
    return (grad_rows, grad_weight, grad_keys, grad_values)


MESH = pl.DeviceIdType.MESH
BF16, F32 = jnp.bfloat16, jnp.float32
NT = (((1,), (1,)), ((), ()))
X = 2
ZS = 4
CHUNK = 512
PIECES = 4


def fused_kernel(
    ts, heads,
    target_hbm, gain_hbm, w_query, queries, keys, values, attn_out, grad_out,
    rows_raw, weight_raw, kv_raw,
    qs, dos, outs, kbuf, vbuf, ktr, delta, sbuf, pbuf, dsbuf, qpart, part_in,
    side_out, side_in, stat, ksum, kv_out, kv_in, kv_tp, sq, ntr, nall,
    dqrow, qt, dqg, wbuf, res_out, rows_out, target, gain, send, recv, local_sem,
):
    rows = queries.shape[0]
    src = keys.shape[0]
    hd = HEAD_DIM
    width = heads * hd
    groups = heads // X
    half = width // X
    gcols = X * rows
    part = src // ts
    feat = target.shape[1] // (ZS * X)
    scale = hd ** (-0.5)
    sp, tp = lax.axis_index("sp"), lax.axis_index("tp")
    z, x = sp // X, sp % X
    core = tp % 2
    side = z // 2
    outer = 1 - (z + side) % 2
    inner = outer == 0
    edge = outer > 0
    z_mate, z_oin, z_oout = 1 + 4 * side - z, 2 - side, 3 - 3 * side
    sib = tp + 1 - 2 * core
    tps = [tp, sib, (tp + 2) % ts, (sib + 2) % ts]
    x_off = 1 - x
    slots_z = [z, z_mate, z_oin, z_oout]
    swap = (1, 0, 2, 3)
    far = 2 + outer

    def dev(zz, xx, tt):
        return (zz * X + xx, tt)

    mate, oin, oout = (dev(a, x, tp) for a in (z_mate, z_oin, z_oout))
    xpeer, y_peer, sib_peer = dev(z, x_off, tp), dev(z, x, tps[2]), dev(z, x, sib)
    counts = {"send": 0, "recv": 0, "local": 0}

    def take(kind, n=1):
        at = counts[kind]
        counts[kind] += n
        return at

    def copy_of(source, dest, device, si, ri):
        return pltpu.make_async_remote_copy(
            src_ref=source, dst_ref=dest, send_sem=send.at[si], recv_sem=recv.at[ri],
            device_id=device, device_id_type=MESH,
        )

    bins = []
    small = {1: take("send"), groups: take("send")}

    def planned(source, dest, device, ri, when):
        size = math.prod(source.shape) * jnp.dtype(source.dtype).itemsize // (2 * width)
        if source.dtype == F32 and source.shape[0] != rows:
            return copy_of(source, dest, device, small[math.prod(source.shape[:-2])], ri)
        for entry in bins:
            if entry["when"] is when and entry["size"] + size <= wbuf.shape[1]:
                break
        else:
            entry = {"when": when, "size": 0, "sem": take("send")}
            bins.append(entry)
        entry["size"] += size
        return copy_of(source, dest, device, entry["sem"], ri)

    def push(source, dest, device, ri, when=None):
        copy = planned(source, dest, device, ri, when)
        if when is None:
            copy.start()
        else:
            pl.when(when)(copy.start)

    def arrived(view, ri):
        copy_of(view, view, xpeer, 0, ri).wait_recv()

    def fetch(source, dest, sem=None):
        sem = take("local") if sem is None else sem
        copy = pltpu.make_async_copy(source, dest, local_sem.at[sem])
        copy.start()
        return copy

    def loaded(view, sem):
        pltpu.make_async_copy(view, view, local_sem.at[sem]).wait()

    barrier = pltpu.get_barrier_semaphore()
    peers = [dev(a, x, tp) for a in slots_z[1:]] + [dev(a, x_off, tp) for a in slots_z]
    peers += [dev(z, xx, t) for xx in (x, x_off) for t in tps[1:]]
    for peer in peers:
        pl.semaphore_signal(barrier, inc=1, device_id=peer, device_id_type=MESH)

    def head_of(g, xx):
        return xx * groups + g

    head_col = pl.ds(pl.multiple_of(tp * hd, hd), hd)
    t_load, gain_load = fetch(target_hbm, target), fetch(gain_hbm, gain)
    q_l, d_l, o_l, w_l = (take("local") for _ in range(4))
    for sem, ref, buf in ((q_l, queries, qs), (d_l, grad_out, dos), (o_l, attn_out, outs)):
        for g in range(groups):
            for xx in range(X):
                view = buf.at[g] if buf is outs else buf.at[g, 0]
                view = view.at[pl.ds(xx * rows, rows)]
                fetch(ref.at[:, pl.ds(head_of(g, xx) * hd, hd)], view, sem)
    k_load = fetch(keys.at[:, head_col], kbuf.at[pl.ds(0, src)])
    v_load = fetch(values.at[:, head_col], vbuf.at[pl.ds(0, src)])
    for e, t in enumerate(tps):
        w_cols = pl.ds(pl.multiple_of(t * width, width), width)
        fetch(w_query.at[:, w_cols], wbuf.at[e], w_l)

    t_load.wait()
    gain_load.wait()
    wide = target[...].astype(F32)
    sq[0] = jnp.broadcast_to(jnp.sum(wide * wide, axis=1, keepdims=True), (rows, 128))
    loaded(dos.at[pl.ds(0, groups), 0], d_l)
    loaded(outs, o_l)
    for g in range(groups):
        dot = jnp.sum(dos[g, 0].astype(F32) * outs[g].astype(F32), axis=1, keepdims=True)
        delta[0, g] = jnp.broadcast_to(dot, (gcols, 128)).T[:1]
    loaded(qs.at[pl.ds(0, groups), 0], q_l)
    k_load.wait()
    v_load.wait()
    pl.semaphore_wait(barrier, len(peers))

    q_r, d_r = take("recv", ZS * groups), take("recv", ZS * groups)
    delta_r, sq_r = take("recv"), take("recv")
    k_r, v_r = take("recv"), take("recv")

    def gather(buf, base, g, a, b, device, when=None):
        push(buf.at[g, a], buf.at[g, b], device, base + ZS * g + b, when)

    push(delta.at[0], delta.at[1], mate, delta_r)
    push(delta.at[0], delta.at[far], oin, delta_r)
    push(delta.at[0], delta.at[far], oout, delta_r)
    for e in range(1, ts):
        push(sq.at[0], sq.at[e], dev(z, x, tps[e]), sq_r)
    gather(qs, q_r, 0, 0, 1, mate)
    gather(qs, q_r, 0, 0, 2, oin, inner)
    push(kbuf.at[pl.ds(0, src)], kbuf.at[pl.ds(src, src)], xpeer, k_r)
    gather(dos, d_r, 0, 0, 1, mate)
    gather(dos, d_r, 0, 0, 2, oin, inner)
    push(vbuf.at[pl.ds(0, src)], vbuf.at[pl.ds(src, src)], xpeer, v_r)
    for g in range(1, groups):
        gather(qs, q_r, g, 0, 1, mate)
        gather(dos, d_r, g, 0, 1, mate)

    ktr[:, :src] = kbuf[:src].T
    arrived(sq.at[pl.ds(1, ts - 1)], sq_r)
    total = sq[0]
    for e in range(1, ts):
        total = total + sq[e]
    inverse = lax.rsqrt(total[:, :1] / (target.shape[1] * ts) + norm_eps)
    normed = target[...].astype(F32) * inverse * gain[...]
    ntr[...] = normed.T.astype(BF16)

    def feature_rows(zz, xx):
        return pl.ds(pl.multiple_of((zz * X + xx) * feat, feat), feat)

    def lanes(slot, xx):
        return pl.ds(pl.multiple_of((slot * X + xx) * rows, rows), rows)

    n_r, n_sib = take("recv"), take("recv")
    n_in = {ts: take("recv"), 2: take("recv"), ts + 2: take("recv")}

    def n_send(zz, slot, xr):
        xx = (x, x_off)[xr]
        push(
            ntr.at[feature_rows(zz, xx)], nall.at[0, :, lanes(slot, x)], dev(zz, xx, tp),
            n_r,
        )

    def n_pass(i, to, device, when=None):
        push(nall.at[i], nall.at[to], device, n_in.get(to, n_sib), when)

    def n_relay(when):
        @pl.when(when)
        def _():
            arrived(nall.at[0], n_in[ts])

        n_pass(ts, ts + 2, y_peer, when)
        n_pass(ts, ts + 1, sib_peer, when)

    nall[0, :, lanes(0, x)] = ntr[feature_rows(z, x)]

    def relay(g, a, b, device):
        for buf, base in ((qs, q_r), (dos, d_r)):
            copy = planned(buf.at[g, a], buf.at[g, b], device, base + ZS * g + b, inner)

            @pl.when(inner)
            def _():
                arrived(buf.at[g, a], base + ZS * g + a)
                copy.start()

    def gathered(g, a):
        @pl.when(edge)
        def _():
            arrived(qs.at[g, a], q_r + ZS * g + a)
            arrived(dos.at[g, a], d_r + ZS * g + a)

    chunks = X * src // CHUNK

    def scores_of(g, j):
        def step(c, peak):
            span = pl.ds(pl.multiple_of(c * CHUNK, CHUNK), CHUNK)
            s = lax.dot_general(kbuf[span], qs[g, j], NT, preferred_element_type=F32)
            sbuf[span] = s
            return jnp.maximum(peak, jnp.max(s, axis=0, keepdims=True))

        return lax.fori_loop(0, chunks, step, jnp.full((1, gcols), -jnp.inf, F32), unroll=True)

    def grads_of(g, j, peak):
        own_delta = delta[j, g]
        lane_span = pl.ds((g * ZS + j) * gcols, gcols)

        def step(c, total):
            span = pl.ds(pl.multiple_of(c * CHUNK, CHUNK), CHUNK)
            p = jnp.exp((sbuf[span] - peak) * scale)
            dp = lax.dot_general(vbuf[span], dos[g, j], NT, preferred_element_type=F32)
            pbuf[span, lane_span] = p.astype(BF16)
            dsbuf[span, lane_span] = (p * (dp - own_delta) * scale).astype(BF16)
            return total + jnp.sum(p, axis=0, keepdims=True)

        total = lax.fori_loop(0, chunks, step, jnp.zeros((1, gcols), F32), unroll=True)
        stat[0, slots_z[j], g, 0:1] = peak * scale
        stat[0, slots_z[j], g, 1:2] = total
        qpart[g, j] = jnp.dot(ktr[...], dsbuf[:, lane_span], preferred_element_type=F32).astype(BF16)

    stat_r = take("recv", groups * (ZS + 1))
    part_r, side_r = take("recv", groups * ZS), take("recv", groups * ZS)

    def mate_stat(g, j):
        return stat_r + (ZS + 1) * g + j

    def share(g, j):
        zt = slots_z[j]
        for device in (oin, oout):
            push(stat.at[0, zt, g], stat.at[far, zt, g], device, mate_stat(g, ZS))
        push(stat.at[0, zt, g], stat.at[1, zt, g], mate, mate_stat(g, j))
        to = swap[j]
        push(qpart.at[g, j], part_in.at[g, to], mate, part_r + ZS * g + to, edge)

    def process(g, j):
        grads_of(g, j, scores_of(g, j))
        share(g, j)

    def weights_of(g, j, sources):
        zt = slots_z[j]
        tops = [stat[e, zt, g, 0:1] for e in sources]
        top = functools.reduce(jnp.maximum, tops)
        scaled = [jnp.exp(m - top) for m in tops]
        summed = sum(f * stat[e, zt, g, 1:2] for e, f in zip(sources, scaled))
        return top, scaled, summed

    def stats_came(g):
        arrived(stat.at[pl.ds(2, 2), pl.ds(0, ZS), g], mate_stat(g, ZS))

    def side_sum(g, j):
        @pl.when(inner)
        def _():
            arrived(stat.at[0, 0, 0], mate_stat(g, swap[j]))
            arrived(part_in.at[g, j], part_r + ZS * g + j)
            _, (f_own, f_mate), _ = weights_of(g, j, (0, 1))
            near_part = qpart[g, j].astype(F32) * f_own + part_in[g, j].astype(F32) * f_mate
            side_out[g, j] = near_part.astype(BF16)

        to = (j + 2) % ZS
        push(side_out.at[g, j], side_in.at[g, to], oin, side_r + ZS * g + to, inner)

    row_r, g_r, xs_r = take("recv", groups), take("recv", groups), take("recv", groups * ZS)
    qt_r, qs_r = take("recv", groups), take("recv", groups)

    def rows_of(slot, xx):
        return pl.ds(pl.multiple_of((slot * X + xx) * rows, rows), rows)

    def lanes_of(xx):
        return pl.ds(pl.multiple_of(xx * hd, hd), hd)

    def spread(g, j, when):
        push(
            dqrow.at[g, j, :, lanes_of(x_off)], dqg.at[g, rows_of(j, x)], xpeer,
            xs_r + ZS * g + j, when,
        )

        @pl.when(when)
        def _():
            dqg[g, rows_of(j, x)] = dqrow[g, j, :, lanes_of(x)]

    def qt_sends(g, when):
        push(dqrow.at[g, 0], qt.at[2, g], y_peer, qt_r + g, when)
        push(dqrow.at[g, 0], qt.at[1, g], sib_peer, qs_r + g, when)

    def reduce_rows(g, j):
        @pl.when(inner)
        def _():
            arrived(side_in.at[g, j], side_r + ZS * g + j)
            top, _, summed = weights_of(g, j, range(ZS))
            near_top, far_top = (weights_of(g, j, pair)[0] for pair in ((0, 1), (2, 3)))
            grad_t = side_out[g, j].astype(F32) * (jnp.exp(near_top - top) / summed)
            grad_t = grad_t + side_in[g, j].astype(F32) * (jnp.exp(far_top - top) / summed)
            grad_own = grad_t.T.astype(BF16)
            for xx in range(X):
                dqrow[g, j, :, pl.ds(xx * hd, hd)] = grad_own[xx * rows : (xx + 1) * rows]

        spread(g, j, inner)
        if j == 0:
            qt_sends(g, inner)

    def joined(g, j):
        arrived(dqg.at[g, pl.ds(0, rows)], xs_r + ZS * g + j)

    def block_of(g, j):
        return dqg.at[g, pl.ds(j * X * rows, X * rows)]

    def hand(g, j):
        @pl.when(inner)
        def _():
            joined(g, j)

        push(block_of(g, j), block_of(g, swap[j]), mate, g_r + g, inner)

    def hand_rows(g):
        push(
            dqrow.at[g, 1, :, lanes_of(x_off)], dqrow.at[g, 0, :, lanes_of(x_off)], mate,
            row_r + g, inner,
        )

    def hand_direct(g):
        for xx in (x_off, x):
            push(
                dqrow.at[g, 1, :, lanes_of(xx)], dqg.at[g, rows_of(0, x)], dev(z_mate, xx, tp),
                g_r + g, inner,
            )

    def dkv():
        pairs = [(g, j) for g in range(groups) for j in range(ZS)]

        def stacked(e, i):
            rows_in = [stat[e, slots_z[j], g, i : i + 1] for g, j in pairs]
            return jnp.concatenate(rows_in, axis=0)

        tops = [stacked(e, 0) for e in range(ZS)]
        top = functools.reduce(jnp.maximum, tops)
        scaled = [jnp.exp(m - top) for m in tops]
        summed = sum(f * stacked(e, 1) for e, f in enumerate(scaled))
        ratios = (scaled[0] / summed).T
        for n in range(0, len(pairs), 2):
            held = []
            for i, buf in enumerate((qs, dos)):
                pieces = [
                    (buf[g, j].astype(F32) * ratios[:, n + k : n + k + 1]).astype(BF16)
                    for k, (g, j) in enumerate(pairs[n : n + 2])
                ]
                held.append(jnp.concatenate(pieces, axis=0))
            span = pl.ds(n * gcols, 2 * gcols)
            for i, left in enumerate((dsbuf, pbuf)):
                piece = jnp.dot(left[:, span], held[i], preferred_element_type=F32)
                ksum[i] = piece if n == 0 else ksum[i] + piece

    kvx_r, kvt_r = take("recv"), take("recv")
    quarter = src // 4
    stores = []

    def kvx(first, last, when):
        for n in range(first, last):
            piece = pl.ds(n % 4 * quarter, quarter)
            push(kv_out.at[n // 4, piece], kv_in.at[n // 4, piece], xpeer, kvx_r, when)

    def part_rows(t):
        return pl.ds(pl.multiple_of(t * part, part), part)

    def kv_finish(when):
        @pl.when(when)
        def _():
            arrived(kv_in, kvx_r)
            for i in range(2):
                kv_tp[i] = (ksum[i, :src] + kv_in[i].astype(F32)).astype(BF16)

        for e in range(1, ts):
            push(
                kv_tp.at[:, part_rows(tps[e])], kv_raw.at[:, :, head_col], dev(z, x, tps[e]),
                kvt_r, when,
            )

    res_r = take("recv")

    def res_push(g, xr, e, when=None):
        k = xr * ts + e
        at = pl.ds(pl.multiple_of(tp * width + x * half + g * hd, hd), hd)
        if k:
            push(
                res_out.at[g, k], weight_raw.at[:, at], dev(z, (x, x_off)[xr], tps[e]),
                res_r, when,
            )
        else:
            stores.append(fetch(res_out.at[g, 0], weight_raw.at[:, at]))

    def project(g):
        for xr in (1, 0):
            block = nall[pl.ds(xr * ts, ts)].reshape(ts * feat, ZS * X * rows)
            result = jnp.dot(block, dqg[g], preferred_element_type=F32).astype(BF16)
            for e in range(ts):
                res_out[g, xr * ts + e] = result[e * feat : (e + 1) * feat]

    def ready(g):
        @pl.when(edge)
        def _():
            arrived(dqg.at[g], g_r + g)

    def own_rows(g):
        @pl.when(edge)
        def _():
            dqrow[g, 0, :, lanes_of(x)] = dqg[g, rows_of(0, x)]
            arrived(dqrow.at[g, 0, :, pl.ds(0, hd)], row_r + g)

        qt_sends(g, edge)

    def qt_pass(g):
        arrived(qt.at[2, g], qt_r + g)
        push(qt.at[2, g], qt.at[3, g], sib_peer, qs_r + g)

    def rows_part(e, g):
        left = dqrow[g, 0] if e == 0 else qt[e, g]
        total = 0.0
        for xx in range(X):
            w_cols = wbuf[e, :, pl.ds(head_of(g, xx) * hd, hd)]
            total = total + lax.dot_general(
                left[:, xx * hd : (xx + 1) * hd], w_cols, NT, preferred_element_type=F32
            )
        return total

    relay(0, 1, 3, oin)
    relay(0, 2, 2, mate)
    for g in range(1, groups):
        gather(qs, q_r, g, 0, 2, oin, inner)
        gather(dos, d_r, g, 0, 2, oin, inner)
    arrived(kbuf.at[pl.ds(src, src)], k_r)
    ktr[:, src:] = kbuf[src:].T
    peak = scores_of(0, 0)
    arrived(vbuf.at[pl.ds(src, src)], v_r)
    relay(1, 1, 3, oin)
    grads_of(0, 0, peak)
    share(0, 0)
    relay(0, 3, 3, mate)
    arrived(delta.at[pl.ds(1, ZS - 1)], delta_r)
    gathered(0, 1)
    process(0, 1)
    for xr in range(X):
        n_send(z_oin, far, xr)
        n_send(z_oout, far, xr)
        n_send(z_mate, 1, xr)
    n_send(z, 0, 1)
    relay(1, 2, 2, mate)
    gathered(0, 2)
    process(0, 2)
    gathered(0, 3)
    process(0, 3)
    side_sum(0, 0)
    side_sum(0, 1)
    relay(1, 3, 3, mate)
    gathered(1, 1)
    side_sum(0, 2)
    arrived(nall.at[0, :, pl.ds(0, (ZS * X - 1) * rows)], n_r)
    n_pass(0, ts, xpeer)
    n_pass(0, 2, y_peer)
    n_pass(0, 1, sib_peer)
    process(1, 0)
    process(1, 1)
    side_sum(0, 3)
    gathered(1, 2)
    process(1, 2)
    n_relay(edge)
    gathered(1, 3)
    process(1, 3)
    @pl.when(inner)
    def _():
        stats_came(0)

    reduce_rows(0, 2)
    reduce_rows(0, 3)
    hand(0, 2)
    n_relay(inner)
    reduce_rows(0, 0)
    hand(0, 3)
    side_sum(1, 0)
    side_sum(1, 1)
    reduce_rows(0, 1)
    hand(0, 0)
    side_sum(1, 2)
    hand(0, 1)
    hand_rows(0)
    side_sum(1, 3)
    arrived(nall.at[0], n_in[2])
    n_pass(2, 3, sib_peer)
    arrived(nall.at[0], n_in[ts + 2])
    n_pass(ts + 2, ts + 3, sib_peer)
    @pl.when(edge)
    def _():
        for g in range(groups):
            for j in range(ZS):
                arrived(stat.at[0, 0, 0], mate_stat(g, j))
            stats_came(g)

    @pl.when(inner)
    def _():
        stats_came(1)

    dkv()
    kv_out[...] = ksum[:, src:].astype(BF16)
    kvx(0, 8, edge)
    reduce_rows(1, 2)
    reduce_rows(1, 3)
    @pl.when(inner)
    def _():
        arrived(nall.at[pl.ds(0, ts)], n_sib)

        project(0)

    for e in (3, 2):
        res_push(0, 1, e, inner)
    hand(1, 2)
    reduce_rows(1, 0)
    hand(1, 3)
    kvx(0, 3, inner)
    for e in (3, 2, 1):
        res_push(0, 0, e, inner)
    @pl.when(edge)
    def _():
        arrived(nall.at[pl.ds(0, ts)], n_sib)

    ready(0)
    @pl.when(edge)
    def _():
        project(0)

    for xr in (1, 0):
        for e in (3, 2, 1, 0):
            if xr or e:
                res_push(0, xr, e, edge)
    res_push(0, 0, 0)
    own_rows(0)
    hand(1, 0)
    reduce_rows(1, 1)
    hand_direct(1)
    hand_rows(1)
    kvx(3, 8, inner)

    @pl.when(inner)
    def _():
        joined(1, 1)

    for e in (1, 0):
        res_push(0, 1, e, inner)
    qt_pass(0)
    kv_finish(edge)
    ready(1)
    own_rows(1)
    project(1)
    for xr in (1, 0):
        for e in (3, 2, 1, 0):
            res_push(1, xr, e)
    kv_finish(inner)
    stores.append(fetch(kv_tp.at[:, part_rows(tp)], kv_raw.at[:, :, head_col]))
    loaded(wbuf, w_l)
    rows_sum = rows_part(0, 0) + rows_part(0, 1) + rows_part(2, 0)
    arrived(qt.at[pl.ds(0, 2), 0], qs_r)
    for e in (1, 3):
        rows_sum = rows_sum + rows_part(e, 0)
    qt_pass(1)
    rows_sum = rows_sum + rows_part(2, 1)
    arrived(qt.at[pl.ds(0, 2), 1], qs_r + 1)
    for e in (1, 3):
        rows_sum = rows_sum + rows_part(e, 1)
    rows_out[...] = rows_sum.astype(BF16)
    stores.append(fetch(rows_out, rows_raw))
    arrived(kv_raw.at[:, :, pl.ds(0, (ts - 1) * hd)], kvt_r)
    arrived(weight_raw.at[:, pl.ds(0, groups * (X * ts - 1) * hd)], res_r)
    for copy in stores:
        copy.wait()
    for sent, sem in ((stat.at[pl.ds(0, ZS - 1)], small[1]), (delta.at[pl.ds(1, ZS - 1)], small[groups])):
        copy_of(sent, sent, xpeer, sem, 0).wait_send()
    for entry in bins:
        sent = wbuf.at[0, pl.ds(0, entry["size"])]
        wait = copy_of(sent, sent, xpeer, entry["sem"], 0).wait_send
        wait() if entry["when"] is None else pl.when(entry["when"])(wait)
    assert counts["send"] <= send.shape[0] and counts["recv"] <= recv.shape[0]


def widen_kernel(
    pieces, rows_raw, weight_raw, kv_raw, grad_rows, grad_weight, grad_keys, grad_values,
    rows_in, weight_in, kv_in, weight_out, kv_out, in_sem, out_sem,
):
    step = weight_raw.shape[0] // pieces
    outs = []

    def start(source, dest, sem):
        copy = pltpu.make_async_copy(source, dest, sem)
        copy.start()
        return copy

    spans = [pl.ds(i * step, step) for i in range(pieces)]
    weight_loads = [
        start(weight_raw.at[span], weight_in.at[span], in_sem.at[3 + i])
        for i, span in enumerate(spans)
    ]
    kv_loads = [start(kv_raw.at[i], kv_in.at[i], in_sem.at[i]) for i in range(2)]
    rows_load = start(rows_raw, rows_in, in_sem.at[2])
    for i, span in enumerate(spans):
        weight_loads[i].wait()
        weight_out[span] = weight_in[span].astype(F32)
        outs.append(start(weight_out.at[span], grad_weight.at[span], out_sem.at[3 + i]))
    for i, out in enumerate((grad_keys, grad_values)):
        kv_loads[i].wait()
        kv_out[i] = kv_in[i].astype(F32)
        outs.append(start(kv_out.at[i], out, out_sem.at[i]))
    rows_load.wait()
    outs.append(start(rows_in, grad_rows, out_sem.at[2]))
    for copy in outs:
        copy.wait()


def fused(target, gain, w_query, queries, keys, values, attn_out, grad_out):
    ts = lax.axis_size("tp")
    rows, width = queries.shape
    src = keys.shape[0]
    heads = width // HEAD_DIM
    hd = HEAD_DIM
    groups, gcols = heads // X, X * rows
    feats = target.shape[1]
    feat = feats // (ZS * X)
    part = src // ts
    hbm = pl.BlockSpec(memory_space=pl.ANY)
    part_shape = pltpu.VMEM((groups, ZS, hd, gcols), BF16)
    raw = pl.pallas_call(
        functools.partial(fused_kernel, ts, heads),
        out_shape=(
            jax.ShapeDtypeStruct((rows, feats), BF16),
            jax.ShapeDtypeStruct((feat, width * ts), BF16),
            jax.ShapeDtypeStruct((2, part, keys.shape[1]), BF16),
        ),
        in_specs=[hbm] * 8,
        out_specs=(hbm,) * 3,
        scratch_shapes=[
            pltpu.VMEM((groups, ZS, gcols, hd), BF16),
            pltpu.VMEM((groups, ZS, gcols, hd), BF16),
            pltpu.VMEM((groups, gcols, hd), BF16),
            pltpu.VMEM((X * src, hd), BF16),
            pltpu.VMEM((X * src, hd), BF16),
            pltpu.VMEM((hd, X * src), BF16),
            pltpu.VMEM((ZS, groups, 1, gcols), F32),
            pltpu.VMEM((X * src, gcols), F32),
            pltpu.VMEM((X * src, groups * ZS * gcols), BF16),
            pltpu.VMEM((X * src, groups * ZS * gcols), BF16),
            part_shape, part_shape, part_shape, part_shape,
            pltpu.VMEM((ZS, ZS, groups, 2, gcols), F32),
            pltpu.VMEM((2, X * src, hd), F32),
            pltpu.VMEM((2, src, hd), BF16),
            pltpu.VMEM((2, src, hd), BF16),
            pltpu.VMEM((2, src, hd), BF16),
            pltpu.VMEM((ts, rows, 128), F32),
            pltpu.VMEM((feats, rows), BF16),
            pltpu.VMEM((X * ts, feat, ZS * X * rows), BF16),
            pltpu.VMEM((groups, ZS, rows, X * hd), BF16),
            pltpu.VMEM((ts, groups, rows, X * hd), BF16),
            pltpu.VMEM((groups, ZS * X * rows, hd), BF16),
            pltpu.VMEM((ts, feats, width), BF16),
            pltpu.VMEM((groups, X * ts, feat, hd), BF16),
            pltpu.VMEM((rows, feats), BF16),
            pltpu.VMEM((rows, feats), BF16),
            pltpu.VMEM((1, feats), F32),
            pltpu.SemaphoreType.DMA((16,)),
            pltpu.SemaphoreType.DMA((76,)),
            pltpu.SemaphoreType.DMA((14,)),
        ],
        compiler_params=pltpu.CompilerParams(
            collective_id=0, has_side_effects=True, vmem_limit_bytes=60 * 2**20
        ),
    )(target, gain.reshape(1, feats), w_query, queries, keys, values, attn_out, grad_out)
    return pl.pallas_call(
        functools.partial(widen_kernel, PIECES),
        out_shape=(
            jax.ShapeDtypeStruct((rows, feats), BF16),
            jax.ShapeDtypeStruct((feat, width * ts), F32),
            jax.ShapeDtypeStruct((part, keys.shape[1]), F32),
            jax.ShapeDtypeStruct((part, keys.shape[1]), F32),
        ),
        in_specs=[hbm] * 3,
        out_specs=(hbm,) * 4,
        scratch_shapes=[
            pltpu.VMEM((rows, feats), BF16),
            pltpu.VMEM((feat, width * ts), BF16),
            pltpu.VMEM((2, part, keys.shape[1]), BF16),
            pltpu.VMEM((feat, width * ts), F32),
            pltpu.VMEM((2, part, keys.shape[1]), F32),
            pltpu.SemaphoreType.DMA((3 + PIECES,)),
            pltpu.SemaphoreType.DMA((3 + PIECES,)),
        ],
    )(*raw)


def fits(mesh):
    sp, tp = mesh.shape["sp"], mesh.shape["tp"]
    feat = WIDTH // (sp * tp)
    heads = HEADS // tp
    return tp == KV_HEADS and sp == ZS * X and feat % 128 == 0 and heads == 2 * X


def solution(mesh):
    return jax.shard_map(
        fused if fits(mesh) else local,
        mesh=mesh,
        in_specs=(
            P("sp", "tp"),
            P("tp"),
            P("tp", None),
            P("sp", "tp"),
            P("sp", None),
            P("sp", None),
            P("sp", "tp"),
            P("sp", "tp"),
        ),
        out_specs=(
            P("sp", "tp"),
            P(("tp", "sp"), None),
            P(("sp", "tp"), None),
            P(("sp", "tp"), None),
        ),
        check_vma=False,
    )
```

```python
import functools
import math

import jax
import jax.numpy as jnp
from jax import lax
from jax.experimental import pallas as pl
from jax.experimental.pallas import tpu as pltpu
from jax.sharding import PartitionSpec as P

WIDTH = 4096
HEADS = 16
KV_HEADS = 4
HEAD_DIM = 256


norm_eps = 1e-06


def merged(part, axis, combine):
    gathered = jax.tree.map(lambda a: lax.all_gather(a, axis), part)

    def take(source):
        return jax.tree.map(lambda a: lax.dynamic_index_in_dim(a, source, 0, False), gathered)

    return lax.fori_loop(
        1, lax.axis_size(axis), lambda source, state: combine(state, take(source)), take(0)
    )


def join_stats(first_part, second_part):
    row_peak = jnp.maximum(first_part[0], second_part[0])
    summed = first_part[1] * jnp.exp(first_part[0] - row_peak) + second_part[1] * jnp.exp(
        second_part[0] - row_peak
    )
    return (row_peak, summed, first_part[2] + second_part[2])


def local(target, gain, w_query, queries, keys, values, attn_out, grad_out):
    local_heads = queries.shape[1] // HEAD_DIM
    group_size = HEADS // KV_HEADS
    score_scale = HEAD_DIM ** (-0.5)
    own_rows = queries.shape[0]
    src_rows = keys.shape[0]
    kv_index = lax.axis_index("tp") * local_heads // group_size
    key_own = lax.dynamic_slice_in_dim(keys, kv_index * HEAD_DIM, HEAD_DIM, 1)
    value_own = lax.dynamic_slice_in_dim(values, kv_index * HEAD_DIM, HEAD_DIM, 1)
    out_heads = attn_out.reshape(own_rows, local_heads, HEAD_DIM).astype(jnp.float32)
    grad_heads = grad_out.reshape(own_rows, local_heads, HEAD_DIM).astype(jnp.float32)
    delta_own = jnp.sum(out_heads * grad_heads, axis=2)
    empty_sum = jnp.zeros((src_rows, HEAD_DIM), jnp.float32)
    total_rows = own_rows * lax.axis_size("sp")
    position = lax.axis_index("sp") * own_rows
    delta_full = lax.dynamic_update_slice_in_dim(
        jnp.zeros((total_rows, local_heads), jnp.float32), delta_own, position, 0
    )
    query_all, grad_all = (
        lax.all_gather(queries, "sp", axis=0, tiled=True),
        lax.all_gather(grad_out, "sp", axis=0, tiled=True),
    )
    block_rows = math.gcd(total_rows, 512)
    block_count = total_rows // block_rows
    query_blocks = query_all.reshape(block_count, block_rows, local_heads, HEAD_DIM)
    grad_blocks = grad_all.reshape(block_count, block_rows, local_heads, HEAD_DIM)

    def block_stats(query_block):
        scores = (
            jnp.einsum("qhd,sd->hqs", query_block, key_own, preferred_element_type=jnp.float32)
            * score_scale
        )
        row_peak = jnp.max(scores, axis=2)
        row_total = jnp.sum(jnp.exp(scores - row_peak[:, :, None]), axis=2)
        return (row_peak, row_total)

    peaks, totals = lax.map(block_stats, query_blocks)
    peaks, totals, delta_full = merged((peaks, totals, delta_full), "sp", join_stats)
    log_totals = peaks + jnp.log(totals)
    delta_blocks = delta_full.reshape(block_count, block_rows, local_heads)

    def block_grads(running, inputs):
        query_block, grad_block, delta_block, log_block = inputs
        scores = (
            jnp.einsum("qhd,sd->hqs", query_block, key_own, preferred_element_type=jnp.float32)
            * score_scale
        )
        weights = jnp.exp(scores - log_block[:, :, None])
        grad_weights = jnp.einsum(
            "qhd,sd->hqs", grad_block, value_own, preferred_element_type=jnp.float32
        )
        delta_cols = jnp.transpose(delta_block)
        grad_scores = (weights * (grad_weights - delta_cols[:, :, None]) * score_scale).astype(
            jnp.bfloat16
        )
        key_sum = running[0] + jnp.einsum(
            "hqs,qhd->sd", grad_scores, query_block, preferred_element_type=jnp.float32
        )
        value_sum = running[1] + jnp.einsum(
            "hqs,qhd->sd",
            weights.astype(jnp.bfloat16),
            grad_block,
            preferred_element_type=jnp.float32,
        )
        query_part = jnp.einsum(
            "hqs,sd->qhd", grad_scores, key_own, preferred_element_type=jnp.float32
        )
        return ((key_sum, value_sum), query_part)

    (key_sum, value_sum), query_parts = lax.scan(
        block_grads, (empty_sum, empty_sum), (query_blocks, grad_blocks, delta_blocks, log_totals)
    )
    query_parts = query_parts.reshape(total_rows, 1, local_heads * HEAD_DIM)
    received = lax.all_to_all(
        query_parts.astype(jnp.bfloat16), "sp", split_axis=0, concat_axis=1, tiled=True
    ).astype(query_parts.dtype)
    query_grad = jnp.sum(received, axis=1)
    key_cols = key_sum.reshape(src_rows, 1, HEAD_DIM)
    value_cols = value_sum.reshape(src_rows, 1, HEAD_DIM)
    key_parts, value_parts = (
        lax.all_to_all(
            key_cols.astype(jnp.bfloat16), "tp", split_axis=0, concat_axis=1, tiled=True
        ).astype(key_cols.dtype),
        lax.all_to_all(
            value_cols.astype(jnp.bfloat16), "tp", split_axis=0, concat_axis=1, tiled=True
        ).astype(value_cols.dtype),
    )
    part_rows = key_parts.shape[0]
    per_kv = key_parts.shape[1] // KV_HEADS
    grad_keys = (
        key_parts.reshape(part_rows, KV_HEADS, per_kv, HEAD_DIM)
        .sum(axis=2)
        .reshape(part_rows, KV_HEADS * HEAD_DIM)
    )
    grad_values = (
        value_parts.reshape(part_rows, KV_HEADS, per_kv, HEAD_DIM)
        .sum(axis=2)
        .reshape(part_rows, KV_HEADS * HEAD_DIM)
    )
    query_grad = query_grad.astype(jnp.bfloat16)
    query_all_heads = lax.all_gather(query_grad, "tp", axis=1, tiled=True)
    grad_rows = lax.dot_general(
        query_all_heads, w_query, (((1,), (1,)), ((), ())), preferred_element_type=jnp.float32
    ).astype(jnp.bfloat16)
    target_wide = target.astype(jnp.float32)
    squares = lax.psum(jnp.sum(target_wide * target_wide, axis=1), "tp")
    inverse = lax.rsqrt(squares / WIDTH + norm_eps)
    normed = (target_wide * inverse[:, None] * gain).astype(jnp.bfloat16)
    grad_weight = lax.psum_scatter(
        lax.dot_general(
            normed, query_all_heads, (((0,), (0,)), ((), ())), preferred_element_type=jnp.float32
        ).astype(jnp.bfloat16),
        "sp",
        scatter_dimension=0,
        tiled=True,
    ).astype(jnp.float32)
    return (grad_rows, grad_weight, grad_keys, grad_values)


MESH = pl.DeviceIdType.MESH
BF16, F32 = jnp.bfloat16, jnp.float32
NT = (((1,), (1,)), ((), ()))
X = 2
ZS = 4
CHUNK = 512
PIECES = 8


def fused_kernel(
    ts, heads,
    target_hbm, gain_hbm, w_query, queries, keys, values, attn_out, grad_out,
    rows_raw, weight_raw, kv_raw,
    qs, dos, outs, kbuf, vbuf, ktr, delta, sbuf, pbuf, dsbuf, qpart, part_in,
    side_out, side_in, stat, ksum, kv_out, kv_in, kv_tp, sq, ntr, nall,
    dqrow, qt, dqg, wbuf, res_out, rows_out, target, gain, send, recv, local_sem,
):
    rows = queries.shape[0]
    src = keys.shape[0]
    hd = HEAD_DIM
    width = heads * hd
    groups = heads // X
    half = width // X
    gcols = X * rows
    part = src // ts
    feat = target.shape[1] // (ZS * X)
    scale = hd ** (-0.5)
    sp, tp = lax.axis_index("sp"), lax.axis_index("tp")
    z, x = sp // X, sp % X
    core = tp % 2
    side = z // 2
    outer = 1 - (z + side) % 2
    inner = outer == 0
    edge = outer > 0
    z_mate, z_oin, z_oout = 1 + 4 * side - z, 2 - side, 3 - 3 * side
    sib = tp + 1 - 2 * core
    tps = [tp, sib, (tp + 2) % ts, (sib + 2) % ts]
    x_off = 1 - x
    slots_z = [z, z_mate, z_oin, z_oout]
    swap = (1, 0, 2, 3)
    far = 2 + outer

    def dev(zz, xx, tt):
        return (zz * X + xx, tt)

    mate, oin, oout = (dev(a, x, tp) for a in (z_mate, z_oin, z_oout))
    xpeer, y_peer, sib_peer = dev(z, x_off, tp), dev(z, x, tps[2]), dev(z, x, sib)
    counts = {"send": 0, "recv": 0, "local": 0}

    def take(kind, n=1):
        at = counts[kind]
        counts[kind] += n
        return at

    def copy_of(source, dest, device, si, ri):
        return pltpu.make_async_remote_copy(
            src_ref=source, dst_ref=dest, send_sem=send.at[si], recv_sem=recv.at[ri],
            device_id=device, device_id_type=MESH,
        )

    bins = []
    small = {1: take("send"), groups: take("send")}

    def planned(source, dest, device, ri, when):
        size = math.prod(source.shape) * jnp.dtype(source.dtype).itemsize // (2 * width)
        if source.dtype == F32 and source.shape[0] != rows:
            return copy_of(source, dest, device, small[math.prod(source.shape[:-2])], ri)
        for entry in bins:
            if entry["when"] is when and entry["size"] + size <= wbuf.shape[1]:
                break
        else:
            entry = {"when": when, "size": 0, "sem": take("send")}
            bins.append(entry)
        entry["size"] += size
        return copy_of(source, dest, device, entry["sem"], ri)

    def push(source, dest, device, ri, when=None):
        copy = planned(source, dest, device, ri, when)
        if when is None:
            copy.start()
        else:
            pl.when(when)(copy.start)

    def arrived(view, ri):
        copy_of(view, view, xpeer, 0, ri).wait_recv()

    def fetch(source, dest, sem=None):
        sem = take("local") if sem is None else sem
        copy = pltpu.make_async_copy(source, dest, local_sem.at[sem])
        copy.start()
        return copy

    def loaded(view, sem):
        pltpu.make_async_copy(view, view, local_sem.at[sem]).wait()

    barrier = pltpu.get_barrier_semaphore()
    peers = [dev(a, x, tp) for a in slots_z[1:]] + [dev(a, x_off, tp) for a in slots_z]
    peers += [dev(z, xx, t) for xx in (x, x_off) for t in tps[1:]]
    for peer in peers:
        pl.semaphore_signal(barrier, inc=1, device_id=peer, device_id_type=MESH)

    def head_of(g, xx):
        return xx * groups + g

    head_col = pl.ds(pl.multiple_of(tp * hd, hd), hd)
    t_load, gain_load = fetch(target_hbm, target), fetch(gain_hbm, gain)
    q_l, d_l, o_l, w_l = (take("local") for _ in range(4))
    for sem, ref, buf in ((q_l, queries, qs), (d_l, grad_out, dos), (o_l, attn_out, outs)):
        for g in range(groups):
            for xx in range(X):
                view = buf.at[g] if buf is outs else buf.at[g, 0]
                view = view.at[pl.ds(xx * rows, rows)]
                fetch(ref.at[:, pl.ds(head_of(g, xx) * hd, hd)], view, sem)
    k_load = fetch(keys.at[:, head_col], kbuf.at[pl.ds(0, src)])
    v_load = fetch(values.at[:, head_col], vbuf.at[pl.ds(0, src)])
    for e, t in enumerate(tps):
        w_cols = pl.ds(pl.multiple_of(t * width, width), width)
        fetch(w_query.at[:, w_cols], wbuf.at[e], w_l)

    t_load.wait()
    gain_load.wait()
    wide = target[...].astype(F32)
    sq[0] = jnp.broadcast_to(jnp.sum(wide * wide, axis=1, keepdims=True), (rows, 128))
    loaded(dos.at[pl.ds(0, groups), 0], d_l)
    loaded(outs, o_l)
    for g in range(groups):
        dot = jnp.sum(dos[g, 0].astype(F32) * outs[g].astype(F32), axis=1, keepdims=True)
        delta[0, g] = jnp.broadcast_to(dot, (gcols, 128)).T[:1]
    loaded(qs.at[pl.ds(0, groups), 0], q_l)
    k_load.wait()
    v_load.wait()
    pl.semaphore_wait(barrier, len(peers))

    q_r, d_r = take("recv", ZS * groups), take("recv", ZS * groups)
    delta_r, sq_r = take("recv"), take("recv")
    k_r, v_r = take("recv"), take("recv")

    def gather(buf, base, g, a, b, device, when=None):
        push(buf.at[g, a], buf.at[g, b], device, base + ZS * g + b, when)

    push(delta.at[0], delta.at[1], mate, delta_r)
    push(delta.at[0], delta.at[far], oin, delta_r)
    push(delta.at[0], delta.at[far], oout, delta_r)
    for e in range(1, ts):
        push(sq.at[0], sq.at[e], dev(z, x, tps[e]), sq_r)
    gather(qs, q_r, 0, 0, 1, mate)
    gather(qs, q_r, 0, 0, 2, oin, inner)
    push(kbuf.at[pl.ds(0, src)], kbuf.at[pl.ds(src, src)], xpeer, k_r)
    gather(dos, d_r, 0, 0, 1, mate)
    gather(dos, d_r, 0, 0, 2, oin, inner)
    push(vbuf.at[pl.ds(0, src)], vbuf.at[pl.ds(src, src)], xpeer, v_r)
    for g in range(1, groups):
        gather(qs, q_r, g, 0, 1, mate)
        gather(dos, d_r, g, 0, 1, mate)

    ktr[:, :src] = kbuf[:src].T
    arrived(sq.at[pl.ds(1, ts - 1)], sq_r)
    total = sq[0]
    for e in range(1, ts):
        total = total + sq[e]
    inverse = lax.rsqrt(total[:, :1] / (target.shape[1] * ts) + norm_eps)
    normed = target[...].astype(F32) * inverse * gain[...]
    ntr[...] = normed.T.astype(BF16)

    def feature_rows(zz, xx):
        return pl.ds(pl.multiple_of((zz * X + xx) * feat, feat), feat)

    def lanes(slot, xx):
        return pl.ds(pl.multiple_of((slot * X + xx) * rows, rows), rows)

    n_r, n_sib = take("recv"), take("recv")
    n_in = {ts: take("recv"), 2: take("recv"), ts + 2: take("recv")}

    def n_send(zz, slot, xr):
        xx = (x, x_off)[xr]
        push(
            ntr.at[feature_rows(zz, xx)], nall.at[0, :, lanes(slot, x)], dev(zz, xx, tp),
            n_r,
        )

    def n_pass(i, to, device, when=None):
        push(nall.at[i], nall.at[to], device, n_in.get(to, n_sib), when)

    def n_relay(when):
        @pl.when(when)
        def _():
            arrived(nall.at[0], n_in[ts])

        n_pass(ts, ts + 2, y_peer, when)
        n_pass(ts, ts + 1, sib_peer, when)

    nall[0, :, lanes(0, x)] = ntr[feature_rows(z, x)]

    def relay(g, a, b, device):
        for buf, base in ((qs, q_r), (dos, d_r)):
            copy = planned(buf.at[g, a], buf.at[g, b], device, base + ZS * g + b, inner)

            @pl.when(inner)
            def _():
                arrived(buf.at[g, a], base + ZS * g + a)
                copy.start()

    def gathered(g, a):
        @pl.when(edge)
        def _():
            arrived(qs.at[g, a], q_r + ZS * g + a)
            arrived(dos.at[g, a], d_r + ZS * g + a)

    chunks = X * src // CHUNK

    def scores_of(g, j):
        def step(c, peak):
            span = pl.ds(pl.multiple_of(c * CHUNK, CHUNK), CHUNK)
            s = lax.dot_general(kbuf[span], qs[g, j], NT, preferred_element_type=F32)
            sbuf[span] = s
            return jnp.maximum(peak, jnp.max(s, axis=0, keepdims=True))

        return lax.fori_loop(0, chunks, step, jnp.full((1, gcols), -jnp.inf, F32), unroll=True)

    def grads_of(g, j, peak):
        own_delta = delta[j, g]
        lane_span = pl.ds((g * ZS + j) * gcols, gcols)

        def step(c, total):
            span = pl.ds(pl.multiple_of(c * CHUNK, CHUNK), CHUNK)
            p = jnp.exp((sbuf[span] - peak) * scale)
            dp = lax.dot_general(vbuf[span], dos[g, j], NT, preferred_element_type=F32)
            pbuf[span, lane_span] = p.astype(BF16)
            dsbuf[span, lane_span] = (p * (dp - own_delta) * scale).astype(BF16)
            return total + jnp.sum(p, axis=0, keepdims=True)

        total = lax.fori_loop(0, chunks, step, jnp.zeros((1, gcols), F32), unroll=True)
        stat[0, slots_z[j], g, 0:1] = peak * scale
        stat[0, slots_z[j], g, 1:2] = total
        qpart[g, j] = jnp.dot(ktr[...], dsbuf[:, lane_span], preferred_element_type=F32).astype(BF16)

    stat_r = take("recv", groups * (ZS + 1))
    part_r, side_r = take("recv", groups * ZS), take("recv", groups * ZS)

    def mate_stat(g, j):
        return stat_r + (ZS + 1) * g + j

    def share(g, j):
        zt = slots_z[j]
        for device in (oin, oout):
            push(stat.at[0, zt, g], stat.at[far, zt, g], device, mate_stat(g, ZS))
        push(stat.at[0, zt, g], stat.at[1, zt, g], mate, mate_stat(g, j))
        to = swap[j]
        push(qpart.at[g, j], part_in.at[g, to], mate, part_r + ZS * g + to, edge)

    def process(g, j):
        grads_of(g, j, scores_of(g, j))
        share(g, j)

    def weights_of(g, j, sources):
        zt = slots_z[j]
        tops = [stat[e, zt, g, 0:1] for e in sources]
        top = functools.reduce(jnp.maximum, tops)
        scaled = [jnp.exp(m - top) for m in tops]
        summed = sum(f * stat[e, zt, g, 1:2] for e, f in zip(sources, scaled))
        return top, scaled, summed

    def stats_came(g):
        arrived(stat.at[pl.ds(2, 2), pl.ds(0, ZS), g], mate_stat(g, ZS))

    def side_sum(g, j):
        @pl.when(inner)
        def _():
            arrived(stat.at[0, 0, 0], mate_stat(g, swap[j]))
            arrived(part_in.at[g, j], part_r + ZS * g + j)
            _, (f_own, f_mate), _ = weights_of(g, j, (0, 1))
            near_part = qpart[g, j].astype(F32) * f_own + part_in[g, j].astype(F32) * f_mate
            side_out[g, j] = near_part.astype(BF16)

        to = (j + 2) % ZS
        push(side_out.at[g, j], side_in.at[g, to], oin, side_r + ZS * g + to, inner)

    row_r, g_r, xs_r = take("recv", groups), take("recv", groups), take("recv", groups * ZS)
    qt_r, qs_r = take("recv", groups), take("recv", groups)

    def rows_of(slot, xx):
        return pl.ds(pl.multiple_of((slot * X + xx) * rows, rows), rows)

    def lanes_of(xx):
        return pl.ds(pl.multiple_of(xx * hd, hd), hd)

    def spread(g, j, when):
        push(
            dqrow.at[g, j, :, lanes_of(x_off)], dqg.at[g, rows_of(j, x)], xpeer,
            xs_r + ZS * g + j, when,
        )

        @pl.when(when)
        def _():
            dqg[g, rows_of(j, x)] = dqrow[g, j, :, lanes_of(x)]

    def qt_sends(g, when):
        push(dqrow.at[g, 0], qt.at[2, g], y_peer, qt_r + g, when)
        push(dqrow.at[g, 0], qt.at[1, g], sib_peer, qs_r + g, when)

    def reduce_rows(g, j):
        @pl.when(inner)
        def _():
            arrived(side_in.at[g, j], side_r + ZS * g + j)
            top, _, summed = weights_of(g, j, range(ZS))
            near_top, far_top = (weights_of(g, j, pair)[0] for pair in ((0, 1), (2, 3)))
            grad_t = side_out[g, j].astype(F32) * (jnp.exp(near_top - top) / summed)
            grad_t = grad_t + side_in[g, j].astype(F32) * (jnp.exp(far_top - top) / summed)
            grad_own = grad_t.T.astype(BF16)
            for xx in range(X):
                dqrow[g, j, :, pl.ds(xx * hd, hd)] = grad_own[xx * rows : (xx + 1) * rows]

        spread(g, j, inner)
        if j == 0:
            qt_sends(g, inner)

    def joined(g, j):
        arrived(dqg.at[g, pl.ds(0, rows)], xs_r + ZS * g + j)

    def block_of(g, j):
        return dqg.at[g, pl.ds(j * X * rows, X * rows)]

    def hand(g, j):
        @pl.when(inner)
        def _():
            joined(g, j)

        push(block_of(g, j), block_of(g, swap[j]), mate, g_r + g, inner)

    def hand_rows(g):
        push(
            dqrow.at[g, 1, :, lanes_of(x_off)], dqrow.at[g, 0, :, lanes_of(x_off)], mate,
            row_r + g, inner,
        )

    def hand_direct(g):
        for xx in (x_off, x):
            push(
                dqrow.at[g, 1, :, lanes_of(xx)], dqg.at[g, rows_of(0, x)], dev(z_mate, xx, tp),
                g_r + g, inner,
            )

    def dkv():
        pairs = [(g, j) for g in range(groups) for j in range(ZS)]

        def stacked(e, i):
            rows_in = [stat[e, slots_z[j], g, i : i + 1] for g, j in pairs]
            return jnp.concatenate(rows_in, axis=0)

        tops = [stacked(e, 0) for e in range(ZS)]
        top = functools.reduce(jnp.maximum, tops)
        scaled = [jnp.exp(m - top) for m in tops]
        summed = sum(f * stacked(e, 1) for e, f in enumerate(scaled))
        ratios = (scaled[0] / summed).T
        for n in range(0, len(pairs), 2):
            held = []
            for i, buf in enumerate((qs, dos)):
                pieces = [
                    (buf[g, j].astype(F32) * ratios[:, n + k : n + k + 1]).astype(BF16)
                    for k, (g, j) in enumerate(pairs[n : n + 2])
                ]
                held.append(jnp.concatenate(pieces, axis=0))
            span = pl.ds(n * gcols, 2 * gcols)
            for i, left in enumerate((dsbuf, pbuf)):
                piece = jnp.dot(left[:, span], held[i], preferred_element_type=F32)
                ksum[i] = piece if n == 0 else ksum[i] + piece

    kvx_r, kvt_r = take("recv"), take("recv")
    quarter = src // 4
    stores = []

    def kvx(first, last, when):
        for n in range(first, last):
            piece = pl.ds(n % 4 * quarter, quarter)
            push(kv_out.at[n // 4, piece], kv_in.at[n // 4, piece], xpeer, kvx_r, when)

    def part_rows(t):
        return pl.ds(pl.multiple_of(t * part, part), part)

    def kv_finish(when):
        @pl.when(when)
        def _():
            arrived(kv_in, kvx_r)
            for i in range(2):
                kv_tp[i] = (ksum[i, :src] + kv_in[i].astype(F32)).astype(BF16)

        for e in range(1, ts):
            push(
                kv_tp.at[:, part_rows(tps[e])], kv_raw.at[:, :, head_col], dev(z, x, tps[e]),
                kvt_r, when,
            )

    res_r = take("recv")

    def res_push(g, xr, e, when=None):
        k = xr * ts + e
        at = pl.ds(pl.multiple_of(tp * width + x * half + g * hd, hd), hd)
        if k:
            push(
                res_out.at[g, k], weight_raw.at[:, at], dev(z, (x, x_off)[xr], tps[e]),
                res_r, when,
            )
        else:
            stores.append(fetch(res_out.at[g, 0], weight_raw.at[:, at]))

    def project(g):
        for xr in (1, 0):
            block = nall[pl.ds(xr * ts, ts)].reshape(ts * feat, ZS * X * rows)
            result = jnp.dot(block, dqg[g], preferred_element_type=F32).astype(BF16)
            for e in range(ts):
                res_out[g, xr * ts + e] = result[e * feat : (e + 1) * feat]

    def ready(g):
        @pl.when(edge)
        def _():
            arrived(dqg.at[g], g_r + g)

    def own_rows(g):
        @pl.when(edge)
        def _():
            dqrow[g, 0, :, lanes_of(x)] = dqg[g, rows_of(0, x)]
            arrived(dqrow.at[g, 0, :, pl.ds(0, hd)], row_r + g)

        qt_sends(g, edge)

    def qt_pass(g):
        arrived(qt.at[2, g], qt_r + g)
        push(qt.at[2, g], qt.at[3, g], sib_peer, qs_r + g)

    def rows_part(e, g):
        left = dqrow[g, 0] if e == 0 else qt[e, g]
        total = 0.0
        for xx in range(X):
            w_cols = wbuf[e, :, pl.ds(head_of(g, xx) * hd, hd)]
            total = total + lax.dot_general(
                left[:, xx * hd : (xx + 1) * hd], w_cols, NT, preferred_element_type=F32
            )
        return total

    relay(0, 1, 3, oin)
    relay(0, 2, 2, mate)
    for g in range(1, groups):
        gather(qs, q_r, g, 0, 2, oin, inner)
        gather(dos, d_r, g, 0, 2, oin, inner)
    arrived(kbuf.at[pl.ds(src, src)], k_r)
    ktr[:, src:] = kbuf[src:].T
    peak = scores_of(0, 0)
    arrived(vbuf.at[pl.ds(src, src)], v_r)
    relay(1, 1, 3, oin)
    grads_of(0, 0, peak)
    share(0, 0)
    relay(0, 3, 3, mate)
    arrived(delta.at[pl.ds(1, ZS - 1)], delta_r)
    gathered(0, 1)
    process(0, 1)
    for xr in range(X):
        n_send(z_oin, far, xr)
        n_send(z_oout, far, xr)
        n_send(z_mate, 1, xr)
    n_send(z, 0, 1)
    relay(1, 2, 2, mate)
    gathered(0, 2)
    process(0, 2)
    gathered(0, 3)
    process(0, 3)
    side_sum(0, 0)
    side_sum(0, 1)
    relay(1, 3, 3, mate)
    gathered(1, 1)
    side_sum(0, 2)
    arrived(nall.at[0, :, pl.ds(0, (ZS * X - 1) * rows)], n_r)
    n_pass(0, ts, xpeer)
    n_pass(0, 2, y_peer)
    n_pass(0, 1, sib_peer)
    process(1, 0)
    process(1, 1)
    side_sum(0, 3)
    gathered(1, 2)
    process(1, 2)
    n_relay(edge)
    gathered(1, 3)
    process(1, 3)
    @pl.when(inner)
    def _():
        stats_came(0)

    reduce_rows(0, 2)
    reduce_rows(0, 3)
    hand(0, 2)
    n_relay(inner)
    reduce_rows(0, 0)
    hand(0, 3)
    side_sum(1, 0)
    side_sum(1, 1)
    reduce_rows(0, 1)
    hand(0, 0)
    side_sum(1, 2)
    hand(0, 1)
    hand_rows(0)
    side_sum(1, 3)
    arrived(nall.at[0], n_in[2])
    n_pass(2, 3, sib_peer)
    arrived(nall.at[0], n_in[ts + 2])
    n_pass(ts + 2, ts + 3, sib_peer)
    @pl.when(edge)
    def _():
        for g in range(groups):
            for j in range(ZS):
                arrived(stat.at[0, 0, 0], mate_stat(g, j))
            stats_came(g)

    @pl.when(inner)
    def _():
        stats_came(1)

    dkv()
    kv_out[...] = ksum[:, src:].astype(BF16)
    kvx(0, 8, edge)
    reduce_rows(1, 2)
    reduce_rows(1, 3)
    @pl.when(inner)
    def _():
        arrived(nall.at[pl.ds(0, ts)], n_sib)

        project(0)

    for e in (3, 2):
        res_push(0, 1, e, inner)
    hand(1, 2)
    reduce_rows(1, 0)
    hand(1, 3)
    kvx(0, 3, inner)
    for e in (3, 2, 1):
        res_push(0, 0, e, inner)
    @pl.when(edge)
    def _():
        arrived(nall.at[pl.ds(0, ts)], n_sib)

    ready(0)
    @pl.when(edge)
    def _():
        project(0)

    for xr in (1, 0):
        for e in (3, 2, 1, 0):
            if xr or e:
                res_push(0, xr, e, edge)
    res_push(0, 0, 0)
    own_rows(0)
    hand(1, 0)
    reduce_rows(1, 1)
    hand_direct(1)
    hand_rows(1)
    kvx(3, 8, inner)

    @pl.when(inner)
    def _():
        joined(1, 1)

    for e in (1, 0):
        res_push(0, 1, e, inner)
    qt_pass(0)
    kv_finish(edge)
    ready(1)
    own_rows(1)
    project(1)
    for xr in (1, 0):
        for e in (3, 2, 1, 0):
            res_push(1, xr, e)
    kv_finish(inner)
    stores.append(fetch(kv_tp.at[:, part_rows(tp)], kv_raw.at[:, :, head_col]))
    loaded(wbuf, w_l)
    rows_sum = rows_part(0, 0) + rows_part(0, 1) + rows_part(2, 0)
    arrived(qt.at[pl.ds(0, 2), 0], qs_r)
    for e in (1, 3):
        rows_sum = rows_sum + rows_part(e, 0)
    qt_pass(1)
    rows_sum = rows_sum + rows_part(2, 1)
    arrived(qt.at[pl.ds(0, 2), 1], qs_r + 1)
    for e in (1, 3):
        rows_sum = rows_sum + rows_part(e, 1)
    rows_out[...] = rows_sum.astype(BF16)
    stores.append(fetch(rows_out, rows_raw))
    arrived(kv_raw.at[:, :, pl.ds(0, (ts - 1) * hd)], kvt_r)
    arrived(weight_raw.at[:, pl.ds(0, groups * (X * ts - 1) * hd)], res_r)
    for copy in stores:
        copy.wait()
    for sent, sem in ((stat.at[pl.ds(0, ZS - 1)], small[1]), (delta.at[pl.ds(1, ZS - 1)], small[groups])):
        copy_of(sent, sent, xpeer, sem, 0).wait_send()
    for entry in bins:
        sent = wbuf.at[0, pl.ds(0, entry["size"])]
        wait = copy_of(sent, sent, xpeer, entry["sem"], 0).wait_send
        wait() if entry["when"] is None else pl.when(entry["when"])(wait)
    assert counts["send"] <= send.shape[0] and counts["recv"] <= recv.shape[0]


def widen_kernel(
    pieces, rows_raw, weight_raw, kv_raw, grad_rows, grad_weight, grad_keys, grad_values,
    rows_in, weight_in, kv_in, weight_out, kv_out, in_sem, out_sem,
):
    step = weight_raw.shape[0] // pieces
    outs = []

    def start(source, dest, sem):
        copy = pltpu.make_async_copy(source, dest, sem)
        copy.start()
        return copy

    spans = [pl.ds(i * step, step) for i in range(pieces)]
    weight_loads = [
        start(weight_raw.at[span], weight_in.at[span], in_sem.at[3 + i])
        for i, span in enumerate(spans)
    ]
    kv_loads = [start(kv_raw.at[i], kv_in.at[i], in_sem.at[i]) for i in range(2)]
    rows_load = start(rows_raw, rows_in, in_sem.at[2])
    for i, span in enumerate(spans):
        weight_loads[i].wait()
        weight_out[span] = weight_in[span].astype(F32)
        outs.append(start(weight_out.at[span], grad_weight.at[span], out_sem.at[3 + i]))
    for i, out in enumerate((grad_keys, grad_values)):
        kv_loads[i].wait()
        kv_out[i] = kv_in[i].astype(F32)
        outs.append(start(kv_out.at[i], out, out_sem.at[i]))
    rows_load.wait()
    outs.append(start(rows_in, grad_rows, out_sem.at[2]))
    for copy in outs:
        copy.wait()


def fused(target, gain, w_query, queries, keys, values, attn_out, grad_out):
    ts = lax.axis_size("tp")
    rows, width = queries.shape
    src = keys.shape[0]
    heads = width // HEAD_DIM
    hd = HEAD_DIM
    groups, gcols = heads // X, X * rows
    feats = target.shape[1]
    feat = feats // (ZS * X)
    part = src // ts
    hbm = pl.BlockSpec(memory_space=pl.ANY)
    part_shape = pltpu.VMEM((groups, ZS, hd, gcols), BF16)
    raw = pl.pallas_call(
        functools.partial(fused_kernel, ts, heads),
        out_shape=(
            jax.ShapeDtypeStruct((rows, feats), BF16),
            jax.ShapeDtypeStruct((feat, width * ts), BF16),
            jax.ShapeDtypeStruct((2, part, keys.shape[1]), BF16),
        ),
        in_specs=[hbm] * 8,
        out_specs=(hbm,) * 3,
        scratch_shapes=[
            pltpu.VMEM((groups, ZS, gcols, hd), BF16),
            pltpu.VMEM((groups, ZS, gcols, hd), BF16),
            pltpu.VMEM((groups, gcols, hd), BF16),
            pltpu.VMEM((X * src, hd), BF16),
            pltpu.VMEM((X * src, hd), BF16),
            pltpu.VMEM((hd, X * src), BF16),
            pltpu.VMEM((ZS, groups, 1, gcols), F32),
            pltpu.VMEM((X * src, gcols), F32),
            pltpu.VMEM((X * src, groups * ZS * gcols), BF16),
            pltpu.VMEM((X * src, groups * ZS * gcols), BF16),
            part_shape, part_shape, part_shape, part_shape,
            pltpu.VMEM((ZS, ZS, groups, 2, gcols), F32),
            pltpu.VMEM((2, X * src, hd), F32),
            pltpu.VMEM((2, src, hd), BF16),
            pltpu.VMEM((2, src, hd), BF16),
            pltpu.VMEM((2, src, hd), BF16),
            pltpu.VMEM((ts, rows, 128), F32),
            pltpu.VMEM((feats, rows), BF16),
            pltpu.VMEM((X * ts, feat, ZS * X * rows), BF16),
            pltpu.VMEM((groups, ZS, rows, X * hd), BF16),
            pltpu.VMEM((ts, groups, rows, X * hd), BF16),
            pltpu.VMEM((groups, ZS * X * rows, hd), BF16),
            pltpu.VMEM((ts, feats, width), BF16),
            pltpu.VMEM((groups, X * ts, feat, hd), BF16),
            pltpu.VMEM((rows, feats), BF16),
            pltpu.VMEM((rows, feats), BF16),
            pltpu.VMEM((1, feats), F32),
            pltpu.SemaphoreType.DMA((16,)),
            pltpu.SemaphoreType.DMA((76,)),
            pltpu.SemaphoreType.DMA((14,)),
        ],
        compiler_params=pltpu.CompilerParams(
            collective_id=0, has_side_effects=True, vmem_limit_bytes=60 * 2**20
        ),
    )(target, gain.reshape(1, feats), w_query, queries, keys, values, attn_out, grad_out)
    return pl.pallas_call(
        functools.partial(widen_kernel, PIECES),
        out_shape=(
            jax.ShapeDtypeStruct((rows, feats), BF16),
            jax.ShapeDtypeStruct((feat, width * ts), F32),
            jax.ShapeDtypeStruct((part, keys.shape[1]), F32),
            jax.ShapeDtypeStruct((part, keys.shape[1]), F32),
        ),
        in_specs=[hbm] * 3,
        out_specs=(hbm,) * 4,
        scratch_shapes=[
            pltpu.VMEM((rows, feats), BF16),
            pltpu.VMEM((feat, width * ts), BF16),
            pltpu.VMEM((2, part, keys.shape[1]), BF16),
            pltpu.VMEM((feat, width * ts), F32),
            pltpu.VMEM((2, part, keys.shape[1]), F32),
            pltpu.SemaphoreType.DMA((3 + PIECES,)),
            pltpu.SemaphoreType.DMA((3 + PIECES,)),
        ],
    )(*raw)


def fits(mesh):
    sp, tp = mesh.shape["sp"], mesh.shape["tp"]
    feat = WIDTH // (sp * tp)
    heads = HEADS // tp
    return tp == KV_HEADS and sp == ZS * X and feat % 128 == 0 and heads == 2 * X


def solution(mesh):
    return jax.shard_map(
        fused if fits(mesh) else local,
        mesh=mesh,
        in_specs=(
            P("sp", "tp"),
            P("tp"),
            P("tp", None),
            P("sp", "tp"),
            P("sp", None),
            P("sp", None),
            P("sp", "tp"),
            P("sp", "tp"),
        ),
        out_specs=(
            P("sp", "tp"),
            P(("tp", "sp"), None),
            P(("sp", "tp"), None),
            P(("sp", "tp"), None),
        ),
        check_vma=False,
    )
```
